128 devices in a mesh: ep: 32 (over z, y, core), tp: 4 (over x).
Axes of the slice: x: 4, y: 4, z: 4, core: 2. Of those that a mesh axis runs over, the one named last changes fastest.
Arguments:
- tokens: bfloat16 [1024, 2048], P('ep'), may hold values from -6 to 6
- kv_cache: bfloat16 [1024, 1024, 512], P('ep', None, 'tp'), may hold values from -320 to 320
- lengths: int32 [1024], P('ep'), may hold values from 1 to 1024, 524288 in all
- attn_gain: float32 [2048], replicated, may hold values from 0.1 to 1.9
- w_query: bfloat16 [2048, 1024], P(None, 'tp'), may hold values from -0.125 to 0.125
- w_key: bfloat16 [2048, 256], P(None, 'tp'), may hold values from -0.125 to 0.125
- w_value: bfloat16 [2048, 256], P(None, 'tp'), may hold values from -0.125 to 0.125
- lambdas: float32 [16], P('tp'), may hold values from 0.3 to 0.8
- head_gain: float32 [64], replicated, may hold values from 0.1 to 1.9
- w_out: bfloat16 [1024, 2048], replicated, may hold values from -0.1875 to 0.1875
- ffn_gain: float32 [2048], replicated, may hold values from 0.1 to 1.9
- w_shared_gate: bfloat16 [2048, 512], P(None, 'tp'), may hold values from -0.125 to 0.125
- w_shared_up: bfloat16 [2048, 512], P(None, 'tp'), may hold values from -0.125 to 0.125
- w_shared_down: bfloat16 [512, 2048], P('tp'), may hold values from -0.25 to 0.25
- routing: int32 [1024, 4], replicated, may hold values from 0 to 127, all different within a row; in each aligned block of 32 rows (0 to 31, 32 to 63, ...) at most 2 rows name the same one
- route_weights: float32 [1024, 4], P('ep'), may hold values from 0.1 to 1
- w_exp_gate: bfloat16 [128, 2048, 512], P(('ep', 'tp')), may hold values from -0.125 to 0.125
- w_exp_up: bfloat16 [128, 2048, 512], P(('ep', 'tp')), may hold values from -0.125 to 0.125
- w_exp_down: bfloat16 [128, 512, 2048], P(('ep', 'tp')), may hold values from -0.25 to 0.25
Outputs:
- mixed: bfloat16 [1024, 2048], P('ep', 'tp')
The draws below stay inside these ranges and needn't reach their ends.
Inputs may be any that keep to these rules, and one draw needn't show every extreme that they name: `lengths`: A sequence's cache holds its past keys and values at positions below its length, and the new token follows them; some sequence uses all 1024 positions. `routing`: each row names 4 different experts. Within the rows of one group of 32 sequences (aligned blocks) no expert is named by more than 2 rows, and in some blocks an expert is named by exactly 2.
All inputs are finite; a program needn't handle non-finite values. No bound on the sum of `lengths` on one device may be relied on, other than what follows from the above.
Results may differ from the reference program's by a relative error of at most 0.015.
The reference program's roundings to bfloat16 on the way count: a program that leaves them out, or rounds other values in their place, can miss the bound.
Values may be sent and summed in bfloat16 or wider, within the bound.
A program may use at most 128 MiB of HBM per device.

```python
import math
import jax
import jax.numpy as jnp
import numpy as np
from jax import lax

D = 2048
HEADS = 16
KV_HEADS = 4
QK_DIM = 32
V_DIM = 64
FF_S = 512
FF_E = 512
TOPK = 4
SEQ_DEV = 32
CACHE = 1024
BATCH = 1024
EXPERTS = 128
CAP = 2
N_EP = 32
N_TP = 4


def draw_kv_cache(key, part):
    key_base = jax.random.fold_in(key, 0)
    full_shape = (BATCH, CACHE, KV_HEADS, 2, 2 * QK_DIM)
    base_draw = jax.random.normal(key_base, full_shape, jnp.float32)
    scales = jnp.array([1.75, 1.0], jnp.float32)
    entries = base_draw * scales[:, None]
    return entries.reshape(BATCH, CACHE, KV_HEADS * 4 * QK_DIM).astype(jnp.bfloat16)


def steps_of(key, dims, cuts, smallest, top_value):
    loudness = 1.0
    for dim, blocks in cuts:
        draws = jax.random.uniform(jax.random.fold_in(jax.random.fold_in(key, 6), dim), (blocks,), jnp.float32, smallest / len(cuts), top_value / len(cuts))
        loudness = loudness * jnp.repeat(jnp.exp(draws), dims[dim] // blocks).reshape((-1,) + (1,) * (len(dims) - 1 - dim))
    return loudness


def split_up(amount, total, reach, slope):
    loads = [(1 << 20) // math.isqrt(grade ** slope) + 1 for grade in range(2, amount + 1)]
    spare, counts = total - reach - (amount - 1), [1] * (amount - 1)
    while spare > 0:
        free = [i for i in range(amount - 1) if counts[i] < reach]
        mass, left = sum([loads[i] for i in free]), spare
        for i in free:
            extra = min(reach - counts[i], max(1, left * loads[i] // mass), spare)
            counts[i] = counts[i] + extra
            spare = spare - extra
    return np.array([reach] + counts)


def ragged_sizes(stream_key, number_of, total, most, lean):
    if number_of == 2:
        one = jax.random.randint(stream_key, (), max(1, total - most), min(most, total - 1) + 1)
        return jnp.stack([one, total - one])
    sizes = jnp.asarray(split_up(number_of, total, most, lean), jnp.int32)
    couples = (number_of - 1) // 2
    giver, taker = sizes[1:1 + 2 * couples:2], sizes[2:2 + 2 * couples:2]
    slack = jnp.minimum(giver - 1, most - taker)
    moved = jax.random.randint(jax.random.fold_in(stream_key, 1), (couples,), 0, 1 << 20) % (slack + 1)
    sizes = sizes.at[1:1 + 2 * couples:2].set(giver - moved).at[2:2 + 2 * couples:2].set(taker + moved)
    return sizes[jax.random.permutation(jax.random.fold_in(stream_key, 2), number_of)]


def shared_out(own_key, own, number, rows, number_of, top, bound, skew):
    sequence = jax.random.permutation(own_key, number_of)
    packed, common = load_shares(number_of, rows * top, bound, skew, True), load_shares(number_of, rows * top, bound, skew, False)
    places = jnp.arange(number_of)

    def named(sizes, rotation):
        used = int((sizes > 0).sum())
        fixed = max(1, used // 4)
        shifted = fixed + (places - fixed + rotation * (used - fixed)) % max(1, number_of - fixed)
        return jnp.zeros((number_of,), jnp.int32).at[sequence[jnp.where(places < fixed, places, shifted)]].set(jnp.asarray(sizes, jnp.int32))

    sizes = jnp.where(number % 4 == 0, named(packed, number // 4), named(common, number - number // 4 - 1))
    mixed = jax.random.permutation(jax.random.fold_in(own, 3), number_of)
    source_of, taker = mixed[0:number_of // 2 * 2:2], mixed[1:number_of // 2 * 2:2]
    room = jnp.minimum(sizes[source_of] - 1, bound - sizes[taker]) // 2
    room = jnp.where((source_of == sequence[0]) | (taker == sequence[0]) | (sizes[taker] == 0), 0, jnp.maximum(room, 0))
    shifted = jax.random.randint(jax.random.fold_in(own, 4), (number_of // 2,), 0, 1 << 20) % (room + 1)
    sizes = sizes.at[source_of].add(-shifted).at[taker].add(shifted)
    labels = jnp.searchsorted(jnp.cumsum(sizes), jnp.arange(rows * top), side="right").astype(jnp.int32)
    table = labels.reshape(top, rows).T
    table = table[jax.random.permutation(jax.random.fold_in(own, 1), rows)]
    rotation = jax.random.randint(jax.random.fold_in(own, 2), (rows, 1), 0, top)
    return jnp.take_along_axis(table, (jnp.arange(top)[None, :] + rotation) % top, axis=1)


def load_shares(count, total, reach, lean, full):
    loads = [(1 << 20) // math.isqrt(rank ** lean) + 1 for rank in range(1, count + 1)]
    largest = reach if full else min(reach, max(-(-total // count), total * loads[0] // sum(loads)))
    least = 1 if total - largest >= count - 1 else 0
    holding, rest = [largest] + [least] * (count - 1), total - largest - least * (count - 1)
    while rest > 0:
        movable = [i for i in range(1, count) if holding[i] < largest] or [i for i in range(1, count) if holding[i] < reach]
        whole, left = sum([loads[i] for i in movable]), rest
        for i in movable:
            extra = min(reach - holding[i], max(1, left * loads[i] // whole), rest)
            holding[i] = holding[i] + extra
            rest = rest - extra
    return np.array(holding)


def normal_values(stream_key, extent, width, bound, cuts=(), kind=jnp.bfloat16):
    drawn = width * jax.random.normal(stream_key, extent, jnp.float32)
    if cuts:
        drawn = drawn * steps_of(stream_key, extent, cuts, -0.22, 0.18)
    return jnp.clip(drawn, -bound, bound).astype(kind)


def setup_inputs(seed: int = 0) -> dict:
    streams_of = jax.random.split(jax.random.key(seed), 20)
    tokens = normal_values(streams_of[0], (BATCH, D), 1.0, 6.0, ((0, 32),))
    kv_cache = draw_kv_cache(jax.random.fold_in(streams_of[19], 71), 0)
    lengths = ragged_sizes(streams_of[2], BATCH, BATCH * CACHE // 2, CACHE, 2).astype(jnp.int32)
    attn_gain = jnp.clip(1.0 + 0.18 * jax.random.normal(streams_of[3], (D,), jnp.float32), 0.1, 1.9)
    w_query = normal_values(streams_of[4], (D, HEADS * 2 * QK_DIM), D ** -0.5, 0.125, ((1, 4),))
    w_key = normal_values(streams_of[5], (D, KV_HEADS * 2 * QK_DIM), D ** -0.5, 0.125, ((1, 4),))
    w_value = normal_values(streams_of[6], (D, KV_HEADS * V_DIM), D ** -0.5, 0.125, ((1, 4),))
    lambdas = jnp.clip(0.3 + 0.5 * jax.random.uniform(streams_of[7], (HEADS,), jnp.float32) ** steps_of(streams_of[7], (HEADS,), ((0, 4),), -0.2, 0.2), 0.3, 0.8)
    head_gain = jnp.clip(1.0 + 0.18 * jax.random.normal(streams_of[8], (V_DIM,), jnp.float32), 0.1, 1.9)
    w_out = normal_values(streams_of[9], (HEADS * V_DIM, D), (HEADS * V_DIM) ** -0.5, 0.1875)
    ffn_gain = jnp.clip(1.0 + 0.18 * jax.random.normal(streams_of[10], (D,), jnp.float32), 0.1, 1.9)
    w_shared_gate = normal_values(streams_of[11], (D, FF_S), D ** -0.5, 0.125, ((1, 4),))
    w_shared_up = normal_values(streams_of[12], (D, FF_S), D ** -0.5, 0.125, ((1, 4),))
    w_shared_down = normal_values(streams_of[13], (FF_S, D), FF_S ** -0.5, 0.25, ((0, 4),))
    routing_keys = jax.random.split(jax.random.fold_in(streams_of[14], 1), BATCH // SEQ_DEV)
    routing_turns = jax.random.permutation(jax.random.fold_in(streams_of[14], 3), BATCH // SEQ_DEV)
    routing = jax.vmap(lambda own, number: shared_out(jax.random.fold_in(streams_of[14], 2), own, number, SEQ_DEV, EXPERTS, TOPK, CAP, 2))(routing_keys, routing_turns).reshape((BATCH, TOPK))
    route_weights = jnp.clip(jnp.exp(math.log(1.0) - 2.3025851 * jax.random.uniform(streams_of[15], (BATCH, TOPK), jnp.float32) ** steps_of(streams_of[15], (BATCH, TOPK), ((0, 32),), -0.2, 0.2)), 0.1, 1.0)
    w_exp_gate = normal_values(streams_of[16], (EXPERTS, D, FF_E), D ** -0.5, 0.125, ((0, 128),))
    w_exp_up = normal_values(streams_of[17], (EXPERTS, D, FF_E), D ** -0.5, 0.125, ((0, 128),))
    w_exp_down = normal_values(streams_of[18], (EXPERTS, FF_E, D), FF_E ** -0.5, 0.25, ((0, 128),))
    return {"tokens": tokens, "kv_cache": kv_cache, "lengths": lengths, "attn_gain": attn_gain, "w_query": w_query, "w_key": w_key, "w_value": w_value, "lambdas": lambdas, "head_gain": head_gain, "w_out": w_out, "ffn_gain": ffn_gain, "w_shared_gate": w_shared_gate, "w_shared_up": w_shared_up, "w_shared_down": w_shared_down, "routing": routing, "route_weights": route_weights, "w_exp_gate": w_exp_gate, "w_exp_up": w_exp_up, "w_exp_down": w_exp_down}


epsilon = 1e-06
neg_fill = -1e+30

def norm_rows(values, gain_vec):
    widened = values.astype(jnp.float32)
    return widened * lax.rsqrt(lax.optimization_barrier(jnp.mean(widened * widened, axis=-1, keepdims=True)) + epsilon) * gain_vec

def group_sum(inner_act, weight):
    row_count = inner_act.shape[0]
    pieces = jnp.einsum('mtf,tfd->mtd', inner_act.reshape(row_count, N_TP, -1).astype(jnp.float32), weight.reshape(N_TP, -1, weight.shape[-1]).astype(jnp.float32))
    rounded = lax.optimization_barrier(pieces.astype(jnp.bfloat16))
    return lax.optimization_barrier(jnp.sum(rounded.astype(jnp.float32), axis=1))

def attend(block_q, block_k, block_v, block_cache, block_len, lambdas, head_gain):
    seq_total = block_q.shape[0]
    v_width = head_gain.shape[0]
    qk_width = v_width // 2
    kv_total = block_cache.shape[2] // (2 * v_width)
    group_size = lambdas.shape[0] // kv_total
    cache_len = block_cache.shape[1]
    queries = block_q.reshape(seq_total, kv_total, group_size, 2, qk_width).astype(jnp.float32)
    key_new = block_k.reshape(seq_total, kv_total, 2, qk_width).astype(jnp.float32)
    value_new = block_v.reshape(seq_total, kv_total, v_width).astype(jnp.float32)
    layout = block_cache.reshape(seq_total, cache_len, kv_total, 2 * v_width)
    keys_old = layout[..., :v_width].reshape(seq_total, cache_len, kv_total, 2, qk_width).astype(jnp.float32)
    values_old = layout[..., v_width:].astype(jnp.float32)
    scaling = qk_width ** (-0.5)
    scores_old = jnp.einsum('skgmd,sckmd->skgmc', queries, keys_old) * scaling
    scores_new = jnp.einsum('skgmd,skmd->skgm', queries, key_new) * scaling
    position = jnp.arange(cache_len, dtype=jnp.int32)
    valid_mask = (position[None, :] < block_len[:, None])[:, None, None, None, :]
    scores_old = jnp.where(valid_mask, scores_old, neg_fill)
    highest = jnp.maximum(lax.optimization_barrier(jnp.max(scores_old, axis=-1)), scores_new)
    expo_old = jnp.where(valid_mask, jnp.exp(scores_old - highest[..., None]), 0.0)
    expo_new = jnp.exp(scores_new - highest)
    totals = lax.optimization_barrier(jnp.sum(expo_old, axis=-1)) + expo_new
    lambda_grid = lambdas.reshape(kv_total, group_size)[None, :, :]
    weight_old = (expo_old[..., 0, :] / totals[..., 0, None] - lambda_grid[..., None] * expo_old[..., 1, :] / totals[..., 1, None]).astype(jnp.bfloat16)
    weight_new = (expo_new[..., 0] / totals[..., 0] - lambda_grid * expo_new[..., 1] / totals[..., 1]).astype(jnp.bfloat16)
    head_mix = jnp.einsum('skgc,sckv->skgv', weight_old.astype(jnp.float32), values_old)
    head_mix = head_mix + weight_new.astype(jnp.float32)[..., None] * value_new[:, :, None, :]
    return norm_rows(head_mix, head_gain).astype(jnp.bfloat16).reshape(seq_total, -1)

def reference(tokens, kv_cache, lengths, attn_gain, w_query, w_key, w_value, lambdas, head_gain, w_out, ffn_gain, w_shared_gate, w_shared_up, w_shared_down, routing, route_weights, w_exp_gate, w_exp_up, w_exp_down):
    normed = norm_rows(tokens, attn_gain).astype(jnp.bfloat16)
    queries = jnp.dot(normed, w_query, preferred_element_type=jnp.float32).astype(jnp.bfloat16)
    key_new = jnp.dot(normed, w_key, preferred_element_type=jnp.float32).astype(jnp.bfloat16)
    value_new = jnp.dot(normed, w_value, preferred_element_type=jnp.float32).astype(jnp.bfloat16)

    def attend_block(operands):
        return attend(operands[0], operands[1], operands[2], operands[3], operands[4], lambdas, head_gain)
    head_out = lax.map(attend_block, (queries.reshape(N_EP, SEQ_DEV, -1), key_new.reshape(N_EP, SEQ_DEV, -1), value_new.reshape(N_EP, SEQ_DEV, -1), kv_cache.reshape(N_EP, SEQ_DEV, CACHE, -1), lengths.reshape(N_EP, SEQ_DEV)))
    head_out = head_out.reshape(BATCH, HEADS * V_DIM)
    projected = group_sum(head_out, w_out)
    residual = (tokens.astype(jnp.float32) + projected).astype(jnp.bfloat16)
    ffn_in = norm_rows(residual, ffn_gain).astype(jnp.bfloat16)
    gate_vals = jnp.dot(ffn_in, w_shared_gate, preferred_element_type=jnp.float32)
    up_vals = jnp.dot(ffn_in, w_shared_up, preferred_element_type=jnp.float32)
    shared_act = (jax.nn.silu(gate_vals) * up_vals).astype(jnp.bfloat16)
    shared = jnp.dot(shared_act, w_shared_down, preferred_element_type=jnp.float32)
    grouped_ids = routing.reshape(N_EP, SEQ_DEV * TOPK)
    onehot = (grouped_ids[..., None] == jnp.arange(EXPERTS, dtype=jnp.int32)).astype(jnp.int32)
    slot_rank = lax.optimization_barrier(jnp.sum((jnp.cumsum(onehot, axis=1) - onehot) * onehot, axis=-1)).astype(jnp.int32)
    group_ids = jnp.broadcast_to(jnp.arange(N_EP, dtype=jnp.int32)[:, None], slot_rank.shape)
    rows_in = jnp.repeat(ffn_in.reshape(N_EP, SEQ_DEV, D), TOPK, axis=1)
    buffers = jnp.zeros((EXPERTS, N_EP, CAP, D), jnp.bfloat16).at[grouped_ids, group_ids, slot_rank].set(rows_in)

    def expert_apply(operands):
        row_block, gate_w, up_w, down_w = operands
        flat_rows = row_block.reshape(N_EP * CAP, D)
        gate_part = jnp.dot(flat_rows, gate_w, preferred_element_type=jnp.float32)
        up_part = jnp.dot(flat_rows, up_w, preferred_element_type=jnp.float32)
        inner_act = (jax.nn.silu(gate_part) * up_part).astype(jnp.bfloat16)
        result = jnp.dot(inner_act, down_w, preferred_element_type=jnp.float32).astype(jnp.bfloat16)
        return result.reshape(N_EP, CAP, D)
    expert_res = lax.map(expert_apply, (buffers, w_exp_gate, w_exp_up, w_exp_down))
    picked = expert_res[grouped_ids, group_ids, slot_rank].astype(jnp.float32)
    routed = lax.optimization_barrier(jnp.sum(route_weights.reshape(N_EP, SEQ_DEV, TOPK, 1) * picked.reshape(N_EP, SEQ_DEV, TOPK, D), axis=2))
    routed = routed.reshape(BATCH, D)
    return (residual.astype(jnp.float32) + shared + routed).astype(jnp.bfloat16)
```

```python
import jax
import jax.numpy as jnp
from jax import lax
from jax.experimental import pallas as pl
from jax.experimental.pallas import tpu as pltpu
from jax.sharding import PartitionSpec as P

MESH = pl.DeviceIdType.MESH
EPS = 1e-06
NEG = -1e30
F32 = jnp.float32
BF16 = jnp.bfloat16
CHUNKS = 4


def iota(shape, dim):
    return lax.broadcasted_iota(jnp.int32, shape, dim)


def dot(a, b):
    return jnp.dot(a, b, preferred_element_type=F32)


def dot_ta(a, b):
    return lax.dot_general(a, b, (((0,), (0,)), ((), ())), preferred_element_type=F32)


def layer(
    n_ep,
    n_tp,
    tokens_h,
    kv_h,
    lengths_s,
    attn_gain_h,
    wq_h,
    wk_h,
    wv_h,
    lambdas_s,
    head_gain_h,
    wo_h,
    ffn_gain_h,
    wsg_h,
    wsu_h,
    wsd_h,
    routing_h,
    rw_h,
    wg_h,
    wu_h,
    wd_h,
    out_ref,
    tokens_v,
    kv_v,
    attn_gain_v,
    wq_v,
    wk_v,
    wv_v,
    head_gain_v,
    wo_v,
    ffn_gain_v,
    wsg_v,
    wsu_v,
    wsd_v,
    routing_v,
    rw_v,
    wg_v,
    wu_v,
    wd_v,
    qblk_v,
    kvn_v,
    sc_v,
    wt_v,
    acc_v,
    ho_v,
    proj_v,
    resid_v,
    oh_v,
    fold_v,
    m2_v,
    send1_v,
    recv1_v,
    shs_v,
    shr_v,
    send2_v,
    recv2_v,
    lsem,
    ksem,
    ho_ss,
    ho_rs,
    d_ss,
    d_rs,
    sh_ss,
    sh_rs,
    r_ss,
    r_rs,
):
    ep = lax.axis_index("ep")
    tp = lax.axis_index("tp")
    n_dev = n_ep * n_tp
    me = ep * n_tp + tp
    seqs, width = tokens_v.shape
    cache = kv_v.shape[1]
    chunk = cache // CHUNKS
    heads = 4
    qk = 32
    rows = heads * seqs

    order = [
        (tokens_h, tokens_v),
        (attn_gain_h, attn_gain_v),
        (wq_h, wq_v),
        (wk_h, wk_v),
        (wv_h, wv_v),
        (routing_h.at[pl.ds(pl.multiple_of(ep * seqs, 8), seqs)], routing_v),
        (rw_h, rw_v),
        (head_gain_h, head_gain_v),
        (ffn_gain_h, ffn_gain_v),
        (wo_h, wo_v),
        (wsg_h, wsg_v),
        (wsu_h, wsu_v),
        (wsd_h, wsd_v),
        (wg_h.at[0], wg_v),
        (wu_h.at[0], wu_v),
        (wd_h.at[0], wd_v),
    ]
    copies = [pltpu.make_async_copy(a, b, lsem.at[i]) for i, (a, b) in enumerate(order)]
    for copy in copies[:9]:
        copy.start()
    kv_copies = []
    for c in range(CHUNKS):
        part = pl.ds(c * chunk, chunk)
        kv_copies.append(
            pltpu.make_async_copy(kv_h.at[:, part, :], kv_v.at[:, part, :], ksem.at[c])
        )
    for copy in kv_copies:
        copy.start()
    for copy in copies[9:]:
        copy.start()

    barrier = pltpu.get_barrier_semaphore()

    def greet(d, carry):
        other = lax.rem(me + d, n_dev)
        pl.semaphore_signal(
            barrier,
            inc=1,
            device_id=(lax.div(other, n_tp), lax.rem(other, n_tp)),
            device_id_type=MESH,
        )
        return carry

    lax.fori_loop(1, n_dev, greet, 0)

    qblk_v[...] = jnp.zeros_like(qblk_v)

    copies[0].wait()
    copies[1].wait()
    tok = tokens_v[...].astype(F32)
    mean = jnp.mean(tok * tok, axis=-1, keepdims=True)
    normed = (tok * lax.rsqrt(mean + EPS) * attn_gain_v[...]).astype(BF16)
    copies[2].wait()
    q = dot(normed, wq_v[...]).astype(BF16)
    copies[3].wait()
    kn = dot(normed, wk_v[...])
    copies[4].wait()
    vn = dot(normed, wv_v[...])
    new_kv = jnp.concatenate([kn, vn], axis=1)

    spread = (
        iota((seqs, heads * rows), 1)
        == iota((seqs, heads * rows), 0)
        + (iota((seqs, heads * rows), 1) // rows) * (rows + seqs)
    ).astype(BF16)
    wide = dot_ta(q, spread)
    qt = wide[0 : 2 * qk, 0:rows]
    for h in range(1, heads):
        qt = qt + wide[h * 2 * qk : (h + 1) * 2 * qk, h * rows : (h + 1) * rows]
    lane_seq = lax.rem(iota((2 * qk, rows), 1), seqs)
    for s in range(seqs):
        block = jnp.where(lane_seq == s, qt, 0.0).astype(BF16)
        qblk_v[s * 128 : s * 128 + qk, 0:rows] = block[0:qk]
        qblk_v[s * 128 + qk : s * 128 + 2 * qk, rows : 2 * rows] = block[qk : 2 * qk]
        kvn_v[s] = jnp.broadcast_to(new_kv[s : s + 1, :], (16, 128)).astype(BF16)

    lane1 = iota((1, 2 * rows), 1)
    len_lane = jnp.zeros((1, 2 * rows), jnp.int32)
    for s in range(seqs):
        len_lane = jnp.where(lax.rem(lane1, seqs) == s, lengths_s[s], len_lane)
    lane_head = iota((1, rows), 1) // seqs
    lam_lane = jnp.zeros((1, rows), F32)
    for h in range(heads):
        lam_lane = jnp.where(lane_head == h, lambdas_s[h], lam_lane)

    lhs_new = jnp.concatenate([kvn_v[s] for s in range(seqs)], axis=1)
    sc_new = dot(lhs_new, qblk_v[...])
    sc_new = jnp.where(iota((16, 2 * rows), 0) == 0, sc_new, NEG)
    top = jnp.max(sc_new, axis=0, keepdims=True)
    for c in range(CHUNKS):
        kv_copies[c].wait()
        part = pl.ds(c * chunk, chunk)
        lhs = jnp.concatenate([kv_v[s, part, :] for s in range(seqs)], axis=1)
        sc = dot(lhs, qblk_v[...])
        valid = iota((chunk, 2 * rows), 0) + c * chunk < len_lane
        sc = jnp.where(valid, sc, NEG)
        sc_v[part, :] = sc
        top = jnp.maximum(top, jnp.max(sc, axis=0, keepdims=True))

    scaling = qk ** (-0.5)
    ex_new = jnp.exp((sc_new - top) * scaling)
    total = jnp.sum(ex_new, axis=0, keepdims=True)
    for c in range(CHUNKS):
        part = pl.ds(c * chunk, chunk)
        ex = jnp.exp((sc_v[part, :] - top) * scaling)
        sc_v[part, :] = ex
        total = total + jnp.sum(ex, axis=0, keepdims=True)
    inv = 1.0 / total
    inv1 = inv[:, 0:rows]
    inv2 = inv[:, rows : 2 * rows] * lam_lane
    w_new = ex_new[:, 0:rows] * inv1 - ex_new[:, rows : 2 * rows] * inv2
    wt_new = jnp.concatenate([w_new, jnp.zeros((112, rows), F32)], axis=0).T.astype(BF16)
    for c in range(CHUNKS):
        part = pl.ds(c * chunk, chunk)
        w = sc_v[part, 0:rows] * inv1 - sc_v[part, rows : 2 * rows] * inv2
        wt_v[:, part] = w.T.astype(BF16)

    acc_v[...] = jnp.zeros_like(acc_v)
    row_seq = lax.rem(iota((rows, 128), 0), seqs)

    def mix(p, carry):
        base = p * 4
        rhs = jnp.concatenate([kv_v[base + i] for i in range(4)], axis=1)
        rhs_new = jnp.concatenate([kvn_v[base + i] for i in range(4)], axis=1)
        o = dot(wt_v[...], rhs) + dot(wt_new[:, 0:16], rhs_new)
        acc = acc_v[...]
        for i in range(4):
            acc = jnp.where(row_seq == base + i, o[:, i * 128 : (i + 1) * 128], acc)
        acc_v[...] = acc
        return carry

    lax.fori_loop(0, seqs // 4, mix, 0)

    upper = iota((rows, 128), 1) >= 64
    mixv = jnp.where(upper, acc_v[...], 0.0)
    copies[7].wait()
    ms = jnp.sum(mixv * mixv, axis=-1, keepdims=True) * (1.0 / 64.0)
    ho = mixv * lax.rsqrt(ms + EPS) * head_gain_v[...]
    low = iota((seqs, 128), 1) < 64
    halves = []
    for i in range(2):
        even = ho[(2 * i) * seqs : (2 * i + 1) * seqs]
        odd = ho[(2 * i + 1) * seqs : (2 * i + 2) * seqs]
        halves.append(jnp.where(low, pltpu.roll(even, 64, 1), odd))
    head_out = jnp.concatenate(halves, axis=1).astype(BF16)
    ho_v[tp] = head_out

    pl.semaphore_wait(barrier, n_dev - 1)
    ho_copies = []
    for d in range(1, n_tp):
        copy = pltpu.make_async_remote_copy(
            src_ref=ho_v.at[tp],
            dst_ref=ho_v.at[tp],
            send_sem=ho_ss.at[d],
            recv_sem=ho_rs.at[d],
            device_id=(ep, lax.rem(tp + d, n_tp)),
            device_id_type=MESH,
        )
        copy.start()
        ho_copies.append(copy)

    copies[5].wait()
    copies[6].wait()
    e_lane = iota((seqs, n_dev), 1)
    picks = [routing_v[:, k : k + 1] for k in range(4)]
    hots = [(e_lane == r).astype(F32) for r in picks]
    named = hots[0] + hots[1] + hots[2] + hots[3]
    earlier = (iota((seqs, seqs), 1) < iota((seqs, seqs), 0)).astype(BF16)
    before = dot(earlier, named.astype(BF16))
    ranks = [jnp.sum(h * before, axis=1, keepdims=True).astype(jnp.int32) for h in hots]
    d_col = iota((seqs, n_ep * 8), 1)
    pieces = []
    for a in range(4):
        piece = jnp.zeros((seqs, n_ep * 8), F32)
        for k in range(4):
            slot = (picks[k] // n_tp) * 8 + ranks[k] * 4 + a
            slot = jnp.where(lax.rem(picks[k], n_tp) == tp, slot, -1)
            piece = piece + (d_col == slot).astype(F32)
        pieces.append(piece)
    oh_v[...] = jnp.concatenate(pieces, axis=0).T.astype(BF16)
    m_col = iota((seqs, n_dev * 8), 1)
    for b in range(4):
        piece = jnp.zeros((seqs, n_dev * 8), F32)
        for k in range(4):
            slot = picks[k] * 8 + ranks[k] * 4 + b
            piece = jnp.where(m_col == slot, rw_v[:, k : k + 1], piece)
        high = piece.astype(BF16)
        m2_v[b * seqs : (b + 1) * seqs, :] = high
        m2_v[(4 + b) * seqs : (5 + b) * seqs, :] = (piece - high.astype(F32)).astype(BF16)
    sq = n_ep * 8
    i0, i1 = iota((sq, sq), 0), iota((sq, sq), 1)
    fold_v[0] = (i1 == lax.rem(i0, sq // 4) * 4 + i0 // (sq // 4)).astype(BF16)
    fold_v[1] = (i1 == lax.rem(i0, 4) * (sq // 4) + i0 // 4).astype(BF16)

    copies[9].wait()
    share = heads * 64

    def project(owner):
        part = dot(ho_v[owner], wo_v[pl.ds(pl.multiple_of(owner * share, share), share), :])
        return part.astype(BF16).astype(F32)

    proj_v[...] = project(tp)
    for d in (1, 3, 2):
        ho_copies[d - 1].wait_recv()
        owner = lax.rem(tp + n_tp - d, n_tp)
        proj_v[...] += project(owner)
    copies[8].wait()
    resid = (tokens_v[...].astype(F32) + proj_v[...]).astype(BF16)
    quarter = width // n_tp
    for t in range(n_tp):
        resid_v[t] = resid[:, t * quarter : (t + 1) * quarter]
    rf = resid.astype(F32)
    mean = jnp.mean(rf * rf, axis=-1, keepdims=True)
    ffn_in = (rf * lax.rsqrt(mean + EPS) * ffn_gain_v[...]).astype(BF16)

    folded = jnp.concatenate(
        [ffn_in[:, a * quarter : (a + 1) * quarter] for a in range(4)], axis=0
    )
    packed = dot(oh_v[...], folded).astype(BF16)
    send1_v[...] = packed.reshape(send1_v.shape)
    recv1_v[ep] = send1_v[ep]

    def dispatch(d, carry):
        other = lax.rem(ep + d, n_ep)
        pltpu.make_async_remote_copy(
            src_ref=send1_v.at[other],
            dst_ref=recv1_v.at[ep],
            send_sem=d_ss,
            recv_sem=d_rs,
            device_id=(other, tp),
            device_id_type=MESH,
        ).start()
        return carry

    lax.fori_loop(1, n_ep, dispatch, 0)

    copies[10].wait()
    copies[11].wait()
    copies[12].wait()
    gate = dot(ffn_in, wsg_v[...])
    up = dot(ffn_in, wsu_v[...])
    act = (gate / (1.0 + jnp.exp(-gate)) * up).astype(BF16)
    part = dot(act, wsd_v[...]).astype(BF16)
    for t in range(n_tp):
        shs_v[t] = part[:, t * quarter : (t + 1) * quarter]
    sh_copies = []
    for d in range(1, n_tp):
        other = lax.rem(tp + d, n_tp)
        copy = pltpu.make_async_remote_copy(
            src_ref=shs_v.at[other],
            dst_ref=shr_v.at[d],
            send_sem=sh_ss.at[d],
            recv_sem=sh_rs.at[d],
            device_id=(ep, other),
            device_id_type=MESH,
        )
        copy.start()
        sh_copies.append(copy)

    copies[13].wait()
    copies[14].wait()
    copies[15].wait()
    arrived = recv1_v.at[pl.ds(0, n_ep - 1)]
    pltpu.make_async_copy(arrived, arrived, d_rs).wait()
    flat = dot(fold_v[0], recv1_v[...].reshape(sq, quarter)).astype(BF16)
    n_rows = sq // 4
    lhs = jnp.concatenate([flat[a * n_rows : (a + 1) * n_rows] for a in range(4)], axis=1)
    gate = dot(lhs, wg_v[...])
    up = dot(lhs, wu_v[...])
    act = (gate / (1.0 + jnp.exp(-gate)) * up).astype(BF16)
    res = dot(act, wd_v[...]).astype(BF16)
    stacked = jnp.concatenate(
        [
            jnp.concatenate(
                [
                    res[:, t * quarter + b * 128 : t * quarter + (b + 1) * 128]
                    for t in range(n_tp)
                ],
                axis=1,
            )
            for b in range(4)
        ],
        axis=0,
    )
    back = dot(fold_v[1], stacked).astype(BF16)
    for t in range(n_tp):
        send2_v[:, t] = back[:, t * 128 : (t + 1) * 128].reshape(n_ep, 8, 128)
    recv2_v[me] = send2_v[ep, tp]

    def give_back(d, carry):
        other = lax.rem(me + d, n_dev)
        oe, ot = lax.div(other, n_tp), lax.rem(other, n_tp)
        pltpu.make_async_remote_copy(
            src_ref=send2_v.at[oe, ot],
            dst_ref=recv2_v.at[me],
            send_sem=r_ss,
            recv_sem=r_rs,
            device_id=(oe, ot),
            device_id_type=MESH,
        ).start()
        return carry

    lax.fori_loop(1, n_dev, give_back, 0)

    final = resid_v[tp].astype(F32) + shs_v[tp].astype(F32)
    for copy in sh_copies:
        copy.wait_recv()
    for d in range(1, n_tp):
        final = final + shr_v[d].astype(F32)
    back_all = recv2_v.at[pl.ds(0, n_dev - 1)]
    pltpu.make_async_copy(back_all, back_all, r_rs).wait()
    routed = dot(m2_v[...], recv2_v[...].reshape(n_dev * 8, 128))
    half = 4 * seqs
    routed = routed[0:half] + routed[half : 2 * half]
    final = final + jnp.concatenate(
        [routed[b * seqs : (b + 1) * seqs] for b in range(4)], axis=1
    )
    out_ref[...] = final.astype(BF16)

    for copy in ho_copies:
        copy.wait_send()
    for copy in sh_copies:
        copy.wait_send()
    sent = send1_v.at[pl.ds(0, n_ep - 1)]
    pltpu.make_async_copy(sent, sent, d_ss).wait()
    pltpu.make_async_copy(back_all, back_all, r_ss).wait()


def solution(mesh):
    n_ep, n_tp = mesh.shape["ep"], mesh.shape["tp"]

    def shards(
        tokens,
        kv_cache,
        lengths,
        attn_gain,
        w_query,
        w_key,
        w_value,
        lambdas,
        head_gain,
        w_out,
        ffn_gain,
        w_shared_gate,
        w_shared_up,
        w_shared_down,
        routing,
        route_weights,
        w_exp_gate,
        w_exp_up,
        w_exp_down,
    ):
        seqs, width = tokens.shape
        n_dev = n_ep * n_tp
        quarter = width // n_tp
        rows = 4 * seqs
        gain2 = jnp.concatenate([head_gain, head_gain]).reshape(1, -1)
        args = (
            tokens,
            kv_cache,
            lengths,
            attn_gain.reshape(1, -1),
            w_query,
            w_key,
            w_value,
            lambdas,
            gain2,
            w_out,
            ffn_gain.reshape(1, -1),
            w_shared_gate,
            w_shared_up,
            w_shared_down,
            routing,
            route_weights,
            w_exp_gate,
            w_exp_up,
            w_exp_down,
        )
        anyspec = pl.BlockSpec(memory_space=pl.ANY)
        smem = pl.BlockSpec(memory_space=pltpu.SMEM)
        specs = [anyspec] * len(args)
        specs[2] = smem
        specs[7] = smem

        def vm(a):
            return pltpu.VMEM(a.shape, a.dtype)

        scratch = [
            vm(tokens),
            vm(kv_cache),
            pltpu.VMEM((1, width), F32),
            vm(w_query),
            vm(w_key),
            vm(w_value),
            pltpu.VMEM((1, 128), F32),
            vm(w_out),
            pltpu.VMEM((1, width), F32),
            vm(w_shared_gate),
            vm(w_shared_up),
            vm(w_shared_down),
            pltpu.VMEM((seqs, 4), jnp.int32),
            vm(route_weights),
            pltpu.VMEM(w_exp_gate.shape[1:], BF16),
            pltpu.VMEM(w_exp_up.shape[1:], BF16),
            pltpu.VMEM(w_exp_down.shape[1:], BF16),
            pltpu.VMEM((seqs * 128, 2 * rows), BF16),
            pltpu.VMEM((seqs, 16, 128), BF16),
            pltpu.VMEM((kv_cache.shape[1], 2 * rows), F32),
            pltpu.VMEM((rows, kv_cache.shape[1]), BF16),
            pltpu.VMEM((rows, 128), F32),
            pltpu.VMEM((n_tp, seqs, 256), BF16),
            pltpu.VMEM((seqs, width), F32),
            pltpu.VMEM((n_tp, seqs, quarter), BF16),
            pltpu.VMEM((n_ep * 8, 4 * seqs), BF16),
            pltpu.VMEM((2, n_ep * 8, n_ep * 8), BF16),
            pltpu.VMEM((8 * seqs, n_dev * 8), BF16),
            pltpu.VMEM((n_ep, 8, quarter), BF16),
            pltpu.VMEM((n_ep, 8, quarter), BF16),
            pltpu.VMEM((n_tp, seqs, quarter), BF16),
            pltpu.VMEM((n_tp, seqs, quarter), BF16),
            pltpu.VMEM((n_ep, n_tp, 8, 128), BF16),
            pltpu.VMEM((n_dev, 8, 128), BF16),
            pltpu.SemaphoreType.DMA((16,)),
            pltpu.SemaphoreType.DMA((CHUNKS,)),
            pltpu.SemaphoreType.DMA((n_tp,)),
            pltpu.SemaphoreType.DMA((n_tp,)),
            pltpu.SemaphoreType.DMA,
            pltpu.SemaphoreType.DMA,
            pltpu.SemaphoreType.DMA((n_tp,)),
            pltpu.SemaphoreType.DMA((n_tp,)),
            pltpu.SemaphoreType.DMA,
            pltpu.SemaphoreType.DMA,
        ]

        def kernel(*refs):
            layer(n_ep, n_tp, *refs)

        return pl.pallas_call(
            kernel,
            name="layer",
            out_shape=jax.ShapeDtypeStruct((seqs, quarter), BF16),
            in_specs=specs,
            out_specs=pl.BlockSpec(memory_space=pltpu.VMEM),
            scratch_shapes=scratch,
            compiler_params=pltpu.CompilerParams(
                collective_id=0, has_side_effects=True, vmem_limit_bytes=66000000
            ),
        )(*args)

    return jax.shard_map(
        shards,
        mesh=mesh,
        in_specs=(
            P("ep", None),
            P("ep", None, "tp"),
            P("ep"),
            P(),
            P(None, "tp"),
            P(None, "tp"),
            P(None, "tp"),
            P("tp"),
            P(),
            P(),
            P(),
            P(None, "tp"),
            P(None, "tp"),
            P("tp", None),
            P(),
            P("ep", None),
            P(("ep", "tp"), None, None),
            P(("ep", "tp"), None, None),
            P(("ep", "tp"), None, None),
        ),
        out_specs=P("ep", "tp"),
        check_vma=False,
    )
```

```python
import jax
import jax.numpy as jnp
from jax import lax
from jax.experimental import pallas as pl
from jax.experimental.pallas import tpu as pltpu
from jax.sharding import PartitionSpec as P

MESH = pl.DeviceIdType.MESH
EPS = 1e-06
NEG = -1e30
F32 = jnp.float32
BF16 = jnp.bfloat16
CHUNKS = 4


def iota(shape, dim):
    return lax.broadcasted_iota(jnp.int32, shape, dim)


def dot(a, b):
    return jnp.dot(a, b, preferred_element_type=F32)


def dot_ta(a, b):
    return lax.dot_general(a, b, (((0,), (0,)), ((), ())), preferred_element_type=F32)


def dot_tb(a, b):
    return lax.dot_general(a, b, (((1,), (1,)), ((), ())), preferred_element_type=F32)


def turned(x):
    tall, wide = x.shape
    if wide < 128:
        x = jnp.concatenate([x, jnp.zeros((tall, 128 - wide), F32)], axis=1)
    return jnp.concatenate([x, jnp.zeros((128 - tall, 128), F32)], axis=0).T


def layer(
    n_ep,
    n_tp,
    tokens_h,
    kv_h,
    lengths_s,
    attn_gain_h,
    wq_h,
    wk_h,
    wv_h,
    lambdas_s,
    head_gain_h,
    wo_h,
    ffn_gain_h,
    wsg_h,
    wsu_h,
    wsd_h,
    routing_h,
    rw_h,
    wg_h,
    wu_h,
    wd_h,
    out_ref,
    tokens_v,
    kv_v,
    attn_gain_v,
    wq_v,
    wkv_v,
    head_gain_v,
    wo_v,
    ffn_gain_v,
    wsg_v,
    wsu_v,
    wsd_v,
    routing_v,
    rw_v,
    table_v,
    wg_v,
    wu_v,
    wd_v,
    qblk_v,
    kvn_v,
    sc_v,
    wt_v,
    ho_v,
    proj_v,
    resid_v,
    oh_v,
    fold_v,
    m2_v,
    send1_v,
    recv1_v,
    shs_v,
    shr_v,
    send2_v,
    recv2_v,
    lsem,
    ksem,
    ho_ss,
    ho_rs,
    d_ss,
    d_rs,
    sh_ss,
    sh_rs,
    r_ss,
    r_rs,
    relay_sem,
):
    ep = lax.axis_index("ep")
    tp = lax.axis_index("tp")
    n_dev = n_ep * n_tp
    me = ep * n_tp + tp
    seqs, width = tokens_v.shape
    cache = kv_v.shape[1]
    chunk = cache // CHUNKS
    heads = 4
    qk = 32
    rows = heads * seqs

    order = [
        (tokens_h, tokens_v),
        (attn_gain_h, attn_gain_v),
        (wq_h, wq_v),
        (wk_h, wkv_v.at[pl.ds(0, 64)]),
        (wv_h, wkv_v.at[pl.ds(64, 64)]),
        (routing_h.at[:, pl.ds(pl.multiple_of(lax.div(ep, 4) * 128, 128), 128)], routing_v),
        (rw_h, rw_v),
        (head_gain_h, head_gain_v),
        (ffn_gain_h, ffn_gain_v),
        (wo_h, wo_v),
        (wsg_h, wsg_v),
        (wsu_h, wsu_v),
        (wsd_h, wsd_v),
        (wg_h.at[0], wg_v),
        (wu_h.at[0], wu_v),
        (wd_h.at[0], wd_v),
    ]
    copies = [pltpu.make_async_copy(a, b, lsem.at[i]) for i, (a, b) in enumerate(order)]
    for copy in copies[:9]:
        copy.start()
    kv_copies = []
    for c in range(CHUNKS):
        part = pl.ds(c * chunk, chunk)
        kv_copies.append(
            pltpu.make_async_copy(kv_h.at[:, part, :], kv_v.at[:, part, :], ksem.at[c])
        )
    for copy in kv_copies:
        copy.start()

    barrier = pltpu.get_barrier_semaphore()

    def greet(d, carry):
        pl.semaphore_signal(
            barrier,
            inc=1,
            device_id=(lax.rem(ep + d, n_ep), tp),
            device_id_type=MESH,
        )
        return carry

    lax.fori_loop(1, n_ep, greet, 0, unroll=True)
    peers = [lax.rem(tp + d, n_tp) for d in range(n_tp)]
    for d in range(1, n_tp):
        pl.semaphore_signal(
            barrier, inc=1, device_id=(ep, peers[d]), device_id_type=MESH
        )

    qblk_v[...] = jnp.zeros_like(qblk_v)

    copies[0].wait()
    copies[1].wait()

    tok = tokens_v[...].astype(F32)
    mean = jnp.mean(tok * tok, axis=-1, keepdims=True)
    normed = (tok * lax.rsqrt(mean + EPS) * attn_gain_v[...]).astype(BF16)
    copies[2].wait()
    q = dot(normed, wq_v[...]).astype(BF16)
    copies[3].wait()
    copies[4].wait()
    new_kv = dot_tb(normed, wkv_v[...])

    spread = (
        iota((seqs, heads * rows), 1)
        == iota((seqs, heads * rows), 0)
        + (iota((seqs, heads * rows), 1) // rows) * (rows + seqs)
    ).astype(BF16)
    wide = dot_ta(q, spread)
    qt = wide[0 : 2 * qk, 0:rows]
    for h in range(1, heads):
        qt = qt + wide[h * 2 * qk : (h + 1) * 2 * qk, h * rows : (h + 1) * rows]
    lane_seq = lax.rem(iota((2 * qk, rows), 1), seqs)
    for s in range(seqs):
        block = jnp.where(lane_seq == s, qt, 0.0).astype(BF16)
        qblk_v[s * 128 : s * 128 + qk, 0:rows] = block[0:qk]
        qblk_v[s * 128 + qk : s * 128 + 2 * qk, rows : 2 * rows] = block[qk : 2 * qk]
        kvn_v[s] = jnp.broadcast_to(new_kv[s : s + 1, :], (16, 128)).astype(BF16)

    lane1 = iota((1, 2 * rows), 1)
    len_lane = jnp.zeros((1, 2 * rows), jnp.int32)
    for s in range(seqs):
        len_lane = jnp.where(lax.rem(lane1, seqs) == s, lengths_s[s], len_lane)
    lane_head = iota((1, rows), 1) // seqs
    lam_lane = jnp.zeros((1, rows), F32)
    for h in range(heads):
        lam_lane = jnp.where(lane_head == h, lambdas_s[h], lam_lane)

    top = jnp.full((1, 2 * rows), NEG, F32)
    for c in range(CHUNKS):
        if c % 2 == 0:
            kv_copies[c].wait()
            kv_copies[c + 1].wait()
        if c == 2:
            for copy in copies[9:]:
                copy.start()
            lhs_new = jnp.concatenate([kvn_v[s] for s in range(seqs)], axis=1)
            sc_new = dot(lhs_new, qblk_v[...])
            sc_new = jnp.where(iota((16, 2 * rows), 0) == 0, sc_new, NEG)
            top = jnp.maximum(top, jnp.max(sc_new, axis=0, keepdims=True))
        part = pl.ds(c * chunk, chunk)
        lhs = jnp.concatenate([kv_v[s, part, :] for s in range(seqs)], axis=1)
        sc = dot(lhs, qblk_v[...])
        valid = iota((chunk, 2 * rows), 0) + c * chunk < len_lane
        sc = jnp.where(valid, sc, NEG)
        sc_v[part, :] = sc
        top = jnp.maximum(top, jnp.max(sc, axis=0, keepdims=True))

    scaling = qk ** (-0.5)
    ex_new = jnp.exp((sc_new - top) * scaling)
    total = jnp.sum(ex_new, axis=0, keepdims=True)
    for c in range(CHUNKS):
        part = pl.ds(c * chunk, chunk)
        ex = jnp.exp((sc_v[part, :] - top) * scaling)
        sc_v[part, :] = ex
        total = total + jnp.sum(ex, axis=0, keepdims=True)
    inv = 1.0 / total
    inv1 = inv[:, 0:rows]
    inv2 = inv[:, rows : 2 * rows] * lam_lane
    w_new = ex_new[:, 0:rows] * inv1 - ex_new[:, rows : 2 * rows] * inv2
    wt_new = jnp.concatenate([w_new, jnp.zeros((112, rows), F32)], axis=0).T.astype(BF16)
    for c in range(CHUNKS):
        part = pl.ds(c * chunk, chunk)
        w = sc_v[part, 0:rows] * inv1 - sc_v[part, rows : 2 * rows] * inv2
        wt_v[:, part] = w.T.astype(BF16)

    acc = jnp.zeros((rows, 128), F32)
    row_seq = lax.rem(iota((rows, 128), 0), seqs)
    for base in range(0, seqs, 4):
        rhs = jnp.concatenate([kv_v[base + i] for i in range(4)], axis=1)
        rhs_new = jnp.concatenate([kvn_v[base + i] for i in range(4)], axis=1)
        o = dot(wt_v[...], rhs) + dot(wt_new[:, 0:16], rhs_new)
        for i in range(4):
            acc = jnp.where(row_seq == base + i, o[:, i * 128 : (i + 1) * 128], acc)

    upper = iota((rows, 128), 1) >= 64
    mixv = jnp.where(upper, acc, 0.0)
    copies[7].wait()
    ms = jnp.sum(mixv * mixv, axis=-1, keepdims=True) * (1.0 / 64.0)
    gain = head_gain_v[...]
    ho = mixv * lax.rsqrt(ms + EPS) * jnp.concatenate([gain, gain], axis=1)
    low = iota((seqs, 128), 1) < 64
    halves = []
    for i in range(2):
        even = ho[(2 * i) * seqs : (2 * i + 1) * seqs]
        odd = ho[(2 * i + 1) * seqs : (2 * i + 2) * seqs]
        halves.append(jnp.where(low, pltpu.roll(even, 64, 1), odd))
    head_out = jnp.concatenate(halves, axis=1).astype(BF16)
    ho_v[tp] = head_out

    pl.semaphore_wait(barrier, n_ep + n_tp - 2)
    ho_copies = []
    for d in range(1, n_tp):
        copy = pltpu.make_async_remote_copy(
            src_ref=ho_v.at[tp],
            dst_ref=ho_v.at[tp],
            send_sem=ho_ss.at[d],
            recv_sem=ho_rs.at[d],
            device_id=(ep, peers[d]),
            device_id_type=MESH,
        )
        copy.start()
        ho_copies.append(copy)
    for d in range(1, n_tp):
        pl.semaphore_signal(
            relay_sem, inc=1, device_id=(ep, peers[d]), device_id_type=MESH
        )

    copies[5].wait()
    copies[6].wait()
    e_lane = iota((seqs, n_dev), 1)
    table_v[...] = turned(routing_v[...].astype(F32))
    own = table_v[pl.ds(pl.multiple_of(lax.rem(ep, 4) * seqs, 8), seqs), :]
    picks = [own[:, k : k + 1].astype(jnp.int32) for k in range(4)]
    rw = turned(rw_v[...])[0:seqs]
    hots = [(e_lane == r).astype(F32) for r in picks]
    named = hots[0] + hots[1] + hots[2] + hots[3]
    earlier = (iota((seqs, seqs), 1) < iota((seqs, seqs), 0)).astype(BF16)
    before = dot(earlier, named.astype(BF16))
    ranks = [jnp.sum(h * before, axis=1, keepdims=True).astype(jnp.int32) for h in hots]
    d_col = iota((seqs, n_ep * 8), 1)
    pieces = []
    for a in range(4):
        piece = jnp.zeros((seqs, n_ep * 8), F32)
        for k in range(4):
            slot = (picks[k] // n_tp) * 8 + ranks[k] * 4 + a
            slot = jnp.where(lax.rem(picks[k], n_tp) == tp, slot, -1)
            piece = piece + (d_col == slot).astype(F32)
        pieces.append(piece)
    oh_v[...] = jnp.concatenate(pieces, axis=0).T.astype(BF16)
    m_col = iota((seqs, n_dev * 8), 1)
    for b in range(4):
        piece = jnp.zeros((seqs, n_dev * 8), F32)
        for k in range(4):
            slot = picks[k] * 8 + ranks[k] * 4 + b
            piece = jnp.where(m_col == slot, rw[:, k : k + 1], piece)
        high = piece.astype(BF16)
        m2_v[b * seqs : (b + 1) * seqs, :] = high
        m2_v[(4 + b) * seqs : (5 + b) * seqs, :] = (piece - high.astype(F32)).astype(BF16)
    sq = n_ep * 8
    i0, i1 = iota((sq, sq), 0), iota((sq, sq), 1)
    fold_v[0] = (i1 == lax.rem(i0, sq // 4) * 4 + i0 // (sq // 4)).astype(BF16)
    fold_v[1] = (i1 == lax.rem(i0, 4) * (sq // 4) + i0 // 4).astype(BF16)

    copies[9].wait()
    share = heads * 64

    def project(owner):
        part = dot(ho_v[owner], wo_v[pl.ds(pl.multiple_of(owner * share, share), share), :])
        return part.astype(BF16).astype(F32)

    proj_v[...] = project(tp)
    for d in (1, 3, 2):
        ho_copies[d - 1].wait_recv()
        owner = lax.rem(tp + n_tp - d, n_tp)
        proj_v[...] += project(owner)
    copies[8].wait()
    resid = (tokens_v[...].astype(F32) + proj_v[...]).astype(BF16)
    quarter = width // n_tp
    for t in range(n_tp):
        resid_v[t] = resid[:, t * quarter : (t + 1) * quarter]
    rf = resid.astype(F32)
    mean = jnp.mean(rf * rf, axis=-1, keepdims=True)
    ffn_in = (rf * lax.rsqrt(mean + EPS) * ffn_gain_v[...]).astype(BF16)

    folded = jnp.concatenate(
        [ffn_in[:, a * quarter : (a + 1) * quarter] for a in range(4)], axis=0
    )
    packed = dot(oh_v[...], folded).astype(BF16)
    send1_v[...] = packed.reshape(send1_v.shape)
    recv1_v[ep] = send1_v[ep]

    def dispatch(d, carry):
        other = lax.rem(ep + d, n_ep)
        pltpu.make_async_remote_copy(
            src_ref=send1_v.at[other],
            dst_ref=recv1_v.at[ep],
            send_sem=d_ss,
            recv_sem=d_rs,
            device_id=(other, tp),
            device_id_type=MESH,
        ).start()
        return carry

    lax.fori_loop(1, n_ep, dispatch, 0)

    copies[10].wait()
    copies[11].wait()
    copies[12].wait()
    gate = dot(ffn_in, wsg_v[...])
    up = dot(ffn_in, wsu_v[...])
    act = (gate / (1.0 + jnp.exp(-gate)) * up).astype(BF16)
    part = dot(act, wsd_v[...]).astype(BF16)
    for t in range(n_tp):
        shs_v[t] = part[:, t * quarter : (t + 1) * quarter]
    sh_copies = []
    for d in range(1, n_tp):
        other = lax.rem(tp + d, n_tp)
        copy = pltpu.make_async_remote_copy(
            src_ref=shs_v.at[other],
            dst_ref=shr_v.at[d],
            send_sem=sh_ss.at[d],
            recv_sem=sh_rs.at[d],
            device_id=(ep, other),
            device_id_type=MESH,
        )
        copy.start()
        sh_copies.append(copy)

    copies[13].wait()
    copies[14].wait()
    copies[15].wait()
    arrived = recv1_v.at[pl.ds(0, n_ep - 1)]
    pltpu.make_async_copy(arrived, arrived, d_rs).wait()
    flat = dot(fold_v[0], recv1_v[...].reshape(sq, quarter)).astype(BF16)
    n_rows = sq // 4
    lhs = jnp.concatenate([flat[a * n_rows : (a + 1) * n_rows] for a in range(4)], axis=1)
    gate = dot(lhs, wg_v[...])
    up = dot(lhs, wu_v[...])
    act = (gate / (1.0 + jnp.exp(-gate)) * up).astype(BF16)
    res = dot(act, wd_v[...]).astype(BF16)
    stacked = jnp.concatenate(
        [
            jnp.concatenate(
                [
                    res[:, t * quarter + b * 128 : t * quarter + (b + 1) * 128]
                    for t in range(n_tp)
                ],
                axis=1,
            )
            for b in range(4)
        ],
        axis=0,
    )
    back = dot(fold_v[1], stacked).astype(BF16)
    for t in range(n_tp):
        send2_v[:, t] = back[:, t * 128 : (t + 1) * 128].reshape(n_ep, 8, 128)
    recv2_v[me] = send2_v[ep, tp]

    pl.semaphore_wait(relay_sem, n_tp - 1)

    def give(oe, ot):
        pltpu.make_async_remote_copy(
            src_ref=send2_v.at[oe, ot],
            dst_ref=recv2_v.at[me],
            send_sem=r_ss,
            recv_sem=r_rs,
            device_id=(oe, ot),
            device_id_type=MESH,
        ).start()

    def give_back(d, carry):
        oe = lax.rem(ep + d, n_ep)
        for ot in peers:
            give(oe, ot)
        return carry

    lax.fori_loop(1, n_ep, give_back, 0)
    for ot in peers[1:]:
        give(ep, ot)

    final = resid_v[tp].astype(F32) + shs_v[tp].astype(F32)
    for copy in sh_copies:
        copy.wait_recv()
    for d in range(1, n_tp):
        final = final + shr_v[d].astype(F32)
    back_all = recv2_v.at[pl.ds(0, n_dev - 1)]
    pltpu.make_async_copy(back_all, back_all, r_rs).wait()
    routed = dot(m2_v[...], recv2_v[...].reshape(n_dev * 8, 128))
    half = 4 * seqs
    routed = routed[0:half] + routed[half : 2 * half]
    final = final + jnp.concatenate(
        [routed[b * seqs : (b + 1) * seqs] for b in range(4)], axis=1
    )
    out_ref[...] = final.astype(BF16)

    for copy in ho_copies:
        copy.wait_send()
    for copy in sh_copies:
        copy.wait_send()
    sent = send1_v.at[pl.ds(0, n_ep - 1)]
    pltpu.make_async_copy(sent, sent, d_ss).wait()
    pltpu.make_async_copy(back_all, back_all, r_ss).wait()


def solution(mesh):
    n_ep, n_tp = mesh.shape["ep"], mesh.shape["tp"]

    def shards(
        tokens,
        kv_cache,
        lengths,
        attn_gain,
        w_query,
        w_key,
        w_value,
        lambdas,
        head_gain,
        w_out,
        ffn_gain,
        w_shared_gate,
        w_shared_up,
        w_shared_down,
        routing,
        route_weights,
        w_exp_gate,
        w_exp_up,
        w_exp_down,
    ):
        seqs, width = tokens.shape
        n_dev = n_ep * n_tp
        quarter = width // n_tp
        rows = 4 * seqs
        args = (
            tokens,
            kv_cache,
            lengths,
            attn_gain.reshape(1, -1),
            w_query,
            w_key.T,
            w_value.T,
            lambdas,
            head_gain.reshape(1, -1),
            w_out,
            ffn_gain.reshape(1, -1),
            w_shared_gate,
            w_shared_up,
            w_shared_down,
            routing.T,
            route_weights.T,
            w_exp_gate,
            w_exp_up,
            w_exp_down,
        )
        anyspec = pl.BlockSpec(memory_space=pltpu.HBM)
        smem = pl.BlockSpec(memory_space=pltpu.SMEM)
        specs = [anyspec] * len(args)
        specs[2] = smem
        specs[7] = smem

        def vm(a):
            return pltpu.VMEM(a.shape, a.dtype)

        scratch = [
            vm(tokens),
            vm(kv_cache),
            pltpu.VMEM((1, width), F32),
            vm(w_query),
            pltpu.VMEM((128, width), BF16),
            pltpu.VMEM((1, 64), F32),
            vm(w_out),
            pltpu.VMEM((1, width), F32),
            vm(w_shared_gate),
            vm(w_shared_up),
            vm(w_shared_down),
            pltpu.VMEM((4, 128), jnp.int32),
            pltpu.VMEM((4, seqs), F32),
            pltpu.VMEM((128, 128), F32),
            pltpu.VMEM(w_exp_gate.shape[1:], BF16),
            pltpu.VMEM(w_exp_up.shape[1:], BF16),
            pltpu.VMEM(w_exp_down.shape[1:], BF16),
            pltpu.VMEM((seqs * 128, 2 * rows), BF16),
            pltpu.VMEM((seqs, 16, 128), BF16),
            pltpu.VMEM((kv_cache.shape[1], 2 * rows), F32),
            pltpu.VMEM((rows, kv_cache.shape[1]), BF16),
            pltpu.VMEM((n_tp, seqs, 256), BF16),
            pltpu.VMEM((seqs, width), F32),
            pltpu.VMEM((n_tp, seqs, quarter), BF16),
            pltpu.VMEM((n_ep * 8, 4 * seqs), BF16),
            pltpu.VMEM((2, n_ep * 8, n_ep * 8), BF16),
            pltpu.VMEM((8 * seqs, n_dev * 8), BF16),
            pltpu.VMEM((n_ep, 8, quarter), BF16),
            pltpu.VMEM((n_ep, 8, quarter), BF16),
            pltpu.VMEM((n_tp, seqs, quarter), BF16),
            pltpu.VMEM((n_tp, seqs, quarter), BF16),
            pltpu.VMEM((n_ep, n_tp, 8, 128), BF16),
            pltpu.VMEM((n_dev, 8, 128), BF16),
            pltpu.SemaphoreType.DMA((16,)),
            pltpu.SemaphoreType.DMA((CHUNKS,)),
            pltpu.SemaphoreType.DMA((n_tp,)),
            pltpu.SemaphoreType.DMA((n_tp,)),
            pltpu.SemaphoreType.DMA,
            pltpu.SemaphoreType.DMA,
            pltpu.SemaphoreType.DMA((n_tp,)),
            pltpu.SemaphoreType.DMA((n_tp,)),
            pltpu.SemaphoreType.DMA,
            pltpu.SemaphoreType.DMA,
            pltpu.SemaphoreType.REGULAR,
        ]

        def kernel(*refs):
            layer(n_ep, n_tp, *refs)

        return pl.pallas_call(
            kernel,
            name="layer",
            out_shape=jax.ShapeDtypeStruct((seqs, quarter), BF16),
            in_specs=specs,
            out_specs=pl.BlockSpec(memory_space=pltpu.VMEM),
            scratch_shapes=scratch,
            compiler_params=pltpu.CompilerParams(
                collective_id=0, has_side_effects=True, vmem_limit_bytes=64000000
            ),
        )(*args)

    return jax.shard_map(
        shards,
        mesh=mesh,
        in_specs=(
            P("ep", None),
            P("ep", None, "tp"),
            P("ep"),
            P(),
            P(None, "tp"),
            P(None, "tp"),
            P(None, "tp"),
            P("tp"),
            P(),
            P(),
            P(),
            P(None, "tp"),
            P(None, "tp"),
            P("tp", None),
            P(),
            P("ep", None),
            P(("ep", "tp"), None, None),
            P(("ep", "tp"), None, None),
            P(("ep", "tp"), None, None),
        ),
        out_specs=P("ep", "tp"),
        check_vma=False,
    )
```

```python
import jax
import jax.numpy as jnp
from jax import lax
from jax.experimental import pallas as pl
from jax.experimental.pallas import tpu as pltpu
from jax.sharding import PartitionSpec as P

MESH = pl.DeviceIdType.MESH
EPS = 1e-06
NEG = -1e30
F32 = jnp.float32
BF16 = jnp.bfloat16
CHUNKS = 4


def iota(shape, dim):
    return lax.broadcasted_iota(jnp.int32, shape, dim)


def dot(a, b):
    return jnp.dot(a, b, preferred_element_type=F32)


def dot_ta(a, b):
    return lax.dot_general(a, b, (((0,), (0,)), ((), ())), preferred_element_type=F32)


def dot_tb(a, b):
    return lax.dot_general(a, b, (((1,), (1,)), ((), ())), preferred_element_type=F32)


def turned(x):
    tall, wide = x.shape
    if wide < 128:
        x = jnp.concatenate([x, jnp.zeros((tall, 128 - wide), F32)], axis=1)
    return jnp.concatenate([x, jnp.zeros((128 - tall, 128), F32)], axis=0).T


def hops(d, n):
    return min(d, n - d)


def layer(
    n_ep,
    n_tp,
    tokens_h,
    kv_h,
    lengths_s,
    attn_gain_h,
    wq_h,
    wk_h,
    wv_h,
    lambdas_s,
    head_gain_h,
    wo_h,
    ffn_gain_h,
    wsg_h,
    wsu_h,
    wsd_h,
    routing_h,
    rw_h,
    wg_h,
    wu_h,
    wd_h,
    out_ref,
    tokens_v,
    kv_v,
    attn_gain_v,
    wq_v,
    wkv_v,
    head_gain_v,
    wo_v,
    ffn_gain_v,
    wsg_v,
    wsu_v,
    wsd_v,
    routing_v,
    rw_v,
    table_v,
    wg_v,
    wu_v,
    wd_v,
    qblk_v,
    kvn_v,
    sc_v,
    wt_v,
    ho_v,
    proj_v,
    resid_v,
    oh_v,
    fold_v,
    m2_v,
    send1_v,
    recv1_v,
    shs_v,
    shr_v,
    send2_v,
    recv2_v,
    lsem,
    ksem,
    ho_ss,
    ho_rs,
    d_ss,
    d_rs,
    sh_ss,
    sh_rs,
    r_ss,
    r_rs,
    relay_sem,
):
    ep = lax.axis_index("ep")
    tp = lax.axis_index("tp")
    n_dev = n_ep * n_tp
    me = ep * n_tp + tp
    seqs, width = tokens_v.shape
    cache = kv_v.shape[1]
    chunk = cache // CHUNKS
    heads = 4
    qk = 32
    rows = heads * seqs
    pairs = seqs // 2

    peers = [lax.rem(tp + d, n_tp) for d in range(n_tp)]
    ez, ey, ec = lax.div(ep, 8), lax.rem(lax.div(ep, 2), 4), lax.rem(ep, 2)
    zs = [lax.rem(ez + d, 4) * 8 for d in range(4)]
    ys = [lax.rem(ey + d, 4) * 2 for d in range(4)]
    cs = [ec, 1 - ec]
    far_peers = sorted(
        (
            (zs[dz] + ys[dy] + cs[dc], hops(dz, 4) + hops(dy, 4))
            for dz in range(4)
            for dy in range(4)
            for dc in range(2)
            if dz + dy + dc
        ),
        key=lambda p: -p[1],
    )
    far_all = sorted(
        (
            (h + hops(d, n_tp), oe, d)
            for oe, h in far_peers + [(ep, 0)]
            for d in range(n_tp)
            if h + d or oe is not ep
        ),
        key=lambda p: -p[0],
    )

    order = [
        (tokens_h, tokens_v),
        (attn_gain_h, attn_gain_v),
        (wq_h, wq_v),
        (wk_h, wkv_v.at[pl.ds(0, 64)]),
        (wv_h, wkv_v.at[pl.ds(64, 64)]),
        (routing_h.at[:, pl.ds(pl.multiple_of(lax.div(ep, 4) * 128, 128), 128)], routing_v),
        (rw_h, rw_v),
        (head_gain_h, head_gain_v),
        (ffn_gain_h, ffn_gain_v),
        (wo_h, wo_v),
        (wsg_h, wsg_v),
        (wsu_h, wsu_v),
        (wsd_h, wsd_v),
        (wg_h.at[0], wg_v),
        (wu_h.at[0], wu_v),
        (wd_h.at[0], wd_v),
    ]
    copies = [pltpu.make_async_copy(a, b, lsem.at[i]) for i, (a, b) in enumerate(order)]
    for copy in copies[:9]:
        copy.start()
    kv_copies = []
    for c in range(CHUNKS):
        part = pl.ds(c * chunk, chunk)
        kv_copies.append(
            pltpu.make_async_copy(kv_h.at[:, part, :], kv_v.at[:, part, :], ksem.at[c])
        )
    for copy in kv_copies:
        copy.start()

    barrier = pltpu.get_barrier_semaphore()

    for other, _ in far_peers:
        pl.semaphore_signal(
            barrier, inc=1, device_id=(other, tp), device_id_type=MESH
        )
    for d in range(1, n_tp):
        pl.semaphore_signal(
            barrier, inc=1, device_id=(ep, peers[d]), device_id_type=MESH
        )

    qblk_v[...] = jnp.zeros_like(qblk_v)

    copies[0].wait()
    copies[1].wait()

    tok = tokens_v[...].astype(F32)
    mean = jnp.mean(tok * tok, axis=-1, keepdims=True)
    normed = (tok * lax.rsqrt(mean + EPS) * attn_gain_v[...]).astype(BF16)
    copies[2].wait()
    q = dot(normed, wq_v[...]).astype(BF16)
    copies[3].wait()
    copies[4].wait()
    new_kv = dot_tb(normed, wkv_v[...])

    spread = (
        iota((seqs, heads * rows), 1)
        == iota((seqs, heads * rows), 0)
        + (iota((seqs, heads * rows), 1) // rows) * (rows + seqs)
    ).astype(BF16)
    wide = dot_ta(q, spread)
    qt = wide[0 : 2 * qk, 0:rows]
    for h in range(1, heads):
        qt = qt + wide[h * 2 * qk : (h + 1) * 2 * qk, h * rows : (h + 1) * rows]
    lane_seq = lax.rem(iota((2 * qk, rows), 1), seqs)
    for s in range(seqs):
        block = jnp.where(lane_seq == s, qt, 0.0).astype(BF16)
        base = s * 2 * qk
        qblk_v[base : base + qk, 0:rows] = block[0:qk]
        qblk_v[base + qk : base + 2 * qk, rows : 2 * rows] = block[qk : 2 * qk]
    low_new = iota((seqs, 128), 1) < 64
    turned_new = pltpu.roll(new_kv, 64, 1)
    k_new = jnp.where(low_new, new_kv, turned_new)
    v_new = jnp.where(low_new, turned_new, new_kv)
    low16 = iota((16, 128), 1) < 64
    for p in range(pairs):
        for i, new in enumerate((k_new, v_new)):
            kvn_v[i, p] = jnp.where(
                low16,
                jnp.broadcast_to(new[2 * p : 2 * p + 1, :], (16, 128)),
                jnp.broadcast_to(new[2 * p + 1 : 2 * p + 2, :], (16, 128)),
            ).astype(BF16)

    lane1 = iota((1, 2 * rows), 1)
    len_lane = jnp.zeros((1, 2 * rows), jnp.int32)
    for s in range(seqs):
        len_lane = jnp.where(lax.rem(lane1, seqs) == s, lengths_s[s], len_lane)
    lane_head = iota((1, rows), 1) // seqs
    lam_lane = jnp.zeros((1, rows), F32)
    for h in range(heads):
        lam_lane = jnp.where(lane_head == h, lambdas_s[h], lam_lane)

    top = jnp.full((1, 2 * rows), NEG, F32)
    part_rows = chunk // 2
    low = iota((part_rows, 128), 1) < 64
    for c in range(CHUNKS):
        kv_copies[c].wait()
        if c == CHUNKS - 1:
            for copy in copies[9:]:
                copy.start()
            lhs_new = jnp.concatenate([kvn_v[0, p] for p in range(pairs)], axis=1)
            sc_new = dot(lhs_new, qblk_v[...])
            sc_new = jnp.where(iota((16, 2 * rows), 0) == 0, sc_new, NEG)
            top = jnp.maximum(top, jnp.max(sc_new, axis=0, keepdims=True))
        for i in range(2):
            start = c * chunk + i * part_rows
            part = pl.ds(start, part_rows)
            lhs = jnp.concatenate(
                [
                    jnp.where(
                        low, kv_v[2 * p, part, :], pltpu.roll(kv_v[2 * p + 1, part, :], 64, 1)
                    )
                    for p in range(pairs)
                ],
                axis=1,
            )
            sc = dot(lhs, qblk_v[...])
            valid = iota((part_rows, 2 * rows), 0) + start < len_lane
            sc = jnp.where(valid, sc, NEG)
            sc_v[part, :] = sc
            top = jnp.maximum(top, jnp.max(sc, axis=0, keepdims=True))

    scaling = qk ** (-0.5)
    ex_new = jnp.exp((sc_new - top) * scaling)
    total = jnp.sum(ex_new, axis=0, keepdims=True)
    for c in range(CHUNKS):
        part = pl.ds(c * chunk, chunk)
        ex = jnp.exp((sc_v[part, :] - top) * scaling)
        sc_v[part, :] = ex
        total = total + jnp.sum(ex, axis=0, keepdims=True)
    inv = 1.0 / total
    inv1 = inv[:, 0:rows]
    inv2 = inv[:, rows : 2 * rows] * lam_lane
    w_new = ex_new[:, 0:rows] * inv1 - ex_new[:, rows : 2 * rows] * inv2
    wt_new = jnp.concatenate([w_new, jnp.zeros((112, rows), F32)], axis=0).T.astype(BF16)
    for c in range(CHUNKS):
        part = pl.ds(c * chunk, chunk)
        w = sc_v[part, 0:rows] * inv1 - sc_v[part, rows : 2 * rows] * inv2
        wt_v[:, part] = w.T.astype(BF16)

    acc = jnp.zeros((rows, 128), F32)
    row_pair = lax.rem(iota((rows, 128), 0), seqs) // 2
    low = iota((cache, 128), 1) < 64
    for base in range(0, pairs, 4):
        rhs = jnp.concatenate(
            [
                jnp.where(low, pltpu.roll(kv_v[2 * p], 64, 1), kv_v[2 * p + 1])
                for p in range(base, base + 4)
            ],
            axis=1,
        )
        rhs_new = jnp.concatenate([kvn_v[1, p] for p in range(base, base + 4)], axis=1)
        o = dot(wt_v[...], rhs) + dot(wt_new[:, 0:16], rhs_new)
        for i in range(4):
            acc = jnp.where(row_pair == base + i, o[:, i * 128 : (i + 1) * 128], acc)

    odd = lax.rem(iota((rows, 128), 0), 2) == 1
    mixv = jnp.where(odd == (iota((rows, 128), 1) >= 64), acc, 0.0)
    copies[7].wait()
    ms = jnp.sum(mixv * mixv, axis=-1, keepdims=True) * (1.0 / 64.0)
    gain = head_gain_v[...]
    mixv = mixv + pltpu.roll(mixv, 64, 1)
    ho = mixv * lax.rsqrt(ms + EPS) * jnp.concatenate([gain, gain], axis=1)
    low = iota((seqs, 128), 1) < 64
    halves = []
    for i in range(2):
        even = ho[(2 * i) * seqs : (2 * i + 1) * seqs]
        odd = ho[(2 * i + 1) * seqs : (2 * i + 2) * seqs]
        halves.append(jnp.where(low, even, odd))
    head_out = jnp.concatenate(halves, axis=1).astype(BF16)
    ho_v[tp] = head_out

    pl.semaphore_wait(barrier, n_ep + n_tp - 2)
    ho_copies = {}
    for d in (2, 1, 3):
        copy = pltpu.make_async_remote_copy(
            src_ref=ho_v.at[tp],
            dst_ref=ho_v.at[tp],
            send_sem=ho_ss.at[d],
            recv_sem=ho_rs.at[d],
            device_id=(ep, peers[d]),
            device_id_type=MESH,
        )
        copy.start()
        ho_copies[d] = copy
    for d in range(1, n_tp):
        pl.semaphore_signal(
            relay_sem, inc=1, device_id=(ep, peers[d]), device_id_type=MESH
        )

    copies[5].wait()
    copies[6].wait()
    e_lane = iota((seqs, n_dev), 1)
    table_v[...] = turned(routing_v[...].astype(F32))
    own = table_v[pl.ds(pl.multiple_of(lax.rem(ep, 4) * seqs, 8), seqs), :]
    picks = [own[:, k : k + 1].astype(jnp.int32) for k in range(4)]
    rw = turned(rw_v[...])[0:seqs]
    hots = [(e_lane == r).astype(F32) for r in picks]
    named = hots[0] + hots[1] + hots[2] + hots[3]
    earlier = (iota((seqs, seqs), 1) < iota((seqs, seqs), 0)).astype(BF16)
    before = dot(earlier, named.astype(BF16))
    ranks = [jnp.sum(h * before, axis=1, keepdims=True).astype(jnp.int32) for h in hots]
    d_col = iota((seqs, n_ep * 8), 1)
    pieces = []
    for a in range(4):
        piece = jnp.zeros((seqs, n_ep * 8), F32)
        for k in range(4):
            slot = (picks[k] // n_tp) * 8 + ranks[k] * 4 + a
            slot = jnp.where(lax.rem(picks[k], n_tp) == tp, slot, -1)
            piece = piece + (d_col == slot).astype(F32)
        pieces.append(piece)
    oh_v[...] = jnp.concatenate(pieces, axis=0).T.astype(BF16)
    m_col = iota((seqs, n_dev * 8), 1)
    for b in range(4):
        piece = jnp.zeros((seqs, n_dev * 8), F32)
        for k in range(4):
            slot = picks[k] * 8 + ranks[k] * 4 + b
            piece = jnp.where(m_col == slot, rw[:, k : k + 1], piece)
        high = piece.astype(BF16)
        m2_v[b * seqs : (b + 1) * seqs, :] = high
        m2_v[(4 + b) * seqs : (5 + b) * seqs, :] = (piece - high.astype(F32)).astype(BF16)
    sq = n_ep * 8
    i0, i1 = iota((sq, sq), 0), iota((sq, sq), 1)
    fold_v[0] = (i1 == lax.rem(i0, sq // 4) * 4 + i0 // (sq // 4)).astype(BF16)
    fold_v[1] = (i1 == lax.rem(i0, 4) * (sq // 4) + i0 // 4).astype(BF16)

    copies[9].wait()
    share = heads * 64

    def project(owner):
        part = dot(ho_v[owner], wo_v[pl.ds(pl.multiple_of(owner * share, share), share), :])
        return part.astype(BF16).astype(F32)

    proj_v[...] = project(tp)
    for d in (1, 3, 2):
        ho_copies[d].wait_recv()
        owner = lax.rem(tp + n_tp - d, n_tp)
        proj_v[...] += project(owner)
    copies[8].wait()
    resid = (tokens_v[...].astype(F32) + proj_v[...]).astype(BF16)
    quarter = width // n_tp
    for t in range(n_tp):
        resid_v[t] = resid[:, t * quarter : (t + 1) * quarter]
    rf = resid.astype(F32)
    mean = jnp.mean(rf * rf, axis=-1, keepdims=True)
    ffn_in = (rf * lax.rsqrt(mean + EPS) * ffn_gain_v[...]).astype(BF16)

    folded = jnp.concatenate(
        [ffn_in[:, a * quarter : (a + 1) * quarter] for a in range(4)], axis=0
    )
    packed = dot(oh_v[...], folded).astype(BF16)
    send1_v[...] = packed.reshape(send1_v.shape)
    recv1_v[ep] = send1_v[ep]

    for other, _ in far_peers:
        pltpu.make_async_remote_copy(
            src_ref=send1_v.at[other],
            dst_ref=recv1_v.at[ep],
            send_sem=d_ss,
            recv_sem=d_rs,
            device_id=(other, tp),
            device_id_type=MESH,
        ).start()

    copies[10].wait()
    copies[11].wait()
    copies[12].wait()
    gate = dot(ffn_in, wsg_v[...])
    up = dot(ffn_in, wsu_v[...])
    act = (gate / (1.0 + jnp.exp(-gate)) * up).astype(BF16)
    part = dot(act, wsd_v[...]).astype(BF16)
    for t in range(n_tp):
        shs_v[t] = part[:, t * quarter : (t + 1) * quarter]
    sh_copies = []
    for d in range(1, n_tp):
        other = lax.rem(tp + d, n_tp)
        copy = pltpu.make_async_remote_copy(
            src_ref=shs_v.at[other],
            dst_ref=shr_v.at[d],
            send_sem=sh_ss.at[d],
            recv_sem=sh_rs.at[d],
            device_id=(ep, other),
            device_id_type=MESH,
        )
        copy.start()
        sh_copies.append(copy)

    copies[13].wait()
    copies[14].wait()
    copies[15].wait()
    arrived = recv1_v.at[pl.ds(0, n_ep - 1)]
    pltpu.make_async_copy(arrived, arrived, d_rs).wait()
    flat = dot(fold_v[0], recv1_v[...].reshape(sq, quarter)).astype(BF16)
    n_rows = sq // 4
    lhs = jnp.concatenate([flat[a * n_rows : (a + 1) * n_rows] for a in range(4)], axis=1)
    gate = dot(lhs, wg_v[...])
    up = dot(lhs, wu_v[...])
    act = (gate / (1.0 + jnp.exp(-gate)) * up).astype(BF16)
    res = dot(act, wd_v[...]).astype(BF16)
    stacked = jnp.concatenate(
        [
            jnp.concatenate(
                [
                    res[:, t * quarter + b * 128 : t * quarter + (b + 1) * 128]
                    for t in range(n_tp)
                ],
                axis=1,
            )
            for b in range(4)
        ],
        axis=0,
    )
    back = dot(fold_v[1], stacked).astype(BF16)
    for t in range(n_tp):
        send2_v[:, t] = back[:, t * 128 : (t + 1) * 128].reshape(n_ep, 8, 128)
    recv2_v[me] = send2_v[ep, tp]

    pl.semaphore_wait(relay_sem, n_tp - 1)

    def give(oe, ot):
        pltpu.make_async_remote_copy(
            src_ref=send2_v.at[oe, ot],
            dst_ref=recv2_v.at[me],
            send_sem=r_ss,
            recv_sem=r_rs,
            device_id=(oe, ot),
            device_id_type=MESH,
        ).start()

    for _, oe, d in far_all:
        give(oe, peers[d])

    final = resid_v[tp].astype(F32) + shs_v[tp].astype(F32)
    for copy in sh_copies:
        copy.wait_recv()
    for d in range(1, n_tp):
        final = final + shr_v[d].astype(F32)
    back_all = recv2_v.at[pl.ds(0, n_dev - 1)]
    pltpu.make_async_copy(back_all, back_all, r_rs).wait()
    routed = dot(m2_v[...], recv2_v[...].reshape(n_dev * 8, 128))
    half = 4 * seqs
    routed = routed[0:half] + routed[half : 2 * half]
    final = final + jnp.concatenate(
        [routed[b * seqs : (b + 1) * seqs] for b in range(4)], axis=1
    )
    out_ref[...] = final.astype(BF16)

    for copy in ho_copies.values():
        copy.wait_send()
    for copy in sh_copies:
        copy.wait_send()
    sent = send1_v.at[pl.ds(0, n_ep - 1)]
    pltpu.make_async_copy(sent, sent, d_ss).wait()
    pltpu.make_async_copy(back_all, back_all, r_ss).wait()


def solution(mesh):
    n_ep, n_tp = mesh.shape["ep"], mesh.shape["tp"]

    def shards(
        tokens,
        kv_cache,
        lengths,
        attn_gain,
        w_query,
        w_key,
        w_value,
        lambdas,
        head_gain,
        w_out,
        ffn_gain,
        w_shared_gate,
        w_shared_up,
        w_shared_down,
        routing,
        route_weights,
        w_exp_gate,
        w_exp_up,
        w_exp_down,
    ):
        seqs, width = tokens.shape
        n_dev = n_ep * n_tp
        quarter = width // n_tp
        rows = 4 * seqs
        args = (
            tokens,
            kv_cache,
            lengths,
            attn_gain.reshape(1, -1),
            w_query,
            w_key.T,
            w_value.T,
            lambdas,
            head_gain.reshape(1, -1),
            w_out,
            ffn_gain.reshape(1, -1),
            w_shared_gate,
            w_shared_up,
            w_shared_down,
            routing.T,
            route_weights.T,
            w_exp_gate,
            w_exp_up,
            w_exp_down,
        )
        anyspec = pl.BlockSpec(memory_space=pltpu.HBM)
        smem = pl.BlockSpec(memory_space=pltpu.SMEM)
        specs = [anyspec] * len(args)
        specs[2] = smem
        specs[7] = smem

        def vm(a):
            return pltpu.VMEM(a.shape, a.dtype)

        scratch = [
            vm(tokens),
            vm(kv_cache),
            pltpu.VMEM((1, width), F32),
            vm(w_query),
            pltpu.VMEM((128, width), BF16),
            pltpu.VMEM((1, 64), F32),
            vm(w_out),
            pltpu.VMEM((1, width), F32),
            vm(w_shared_gate),
            vm(w_shared_up),
            vm(w_shared_down),
            pltpu.VMEM((4, 128), jnp.int32),
            pltpu.VMEM((4, seqs), F32),
            pltpu.VMEM((128, 128), F32),
            pltpu.VMEM(w_exp_gate.shape[1:], BF16),
            pltpu.VMEM(w_exp_up.shape[1:], BF16),
            pltpu.VMEM(w_exp_down.shape[1:], BF16),
            pltpu.VMEM((seqs * 64, 2 * rows), BF16),
            pltpu.VMEM((2, seqs // 2, 16, 128), BF16),
            pltpu.VMEM((kv_cache.shape[1], 2 * rows), F32),
            pltpu.VMEM((rows, kv_cache.shape[1]), BF16),
            pltpu.VMEM((n_tp, seqs, 256), BF16),
            pltpu.VMEM((seqs, width), F32),
            pltpu.VMEM((n_tp, seqs, quarter), BF16),
            pltpu.VMEM((n_ep * 8, 4 * seqs), BF16),
            pltpu.VMEM((2, n_ep * 8, n_ep * 8), BF16),
            pltpu.VMEM((8 * seqs, n_dev * 8), BF16),
            pltpu.VMEM((n_ep, 8, quarter), BF16),
            pltpu.VMEM((n_ep, 8, quarter), BF16),
            pltpu.VMEM((n_tp, seqs, quarter), BF16),
            pltpu.VMEM((n_tp, seqs, quarter), BF16),
            pltpu.VMEM((n_ep, n_tp, 8, 128), BF16),
            pltpu.VMEM((n_dev, 8, 128), BF16),
            pltpu.SemaphoreType.DMA((16,)),
            pltpu.SemaphoreType.DMA((CHUNKS,)),
            pltpu.SemaphoreType.DMA((n_tp,)),
            pltpu.SemaphoreType.DMA((n_tp,)),
            pltpu.SemaphoreType.DMA,
            pltpu.SemaphoreType.DMA,
            pltpu.SemaphoreType.DMA((n_tp,)),
            pltpu.SemaphoreType.DMA((n_tp,)),
            pltpu.SemaphoreType.DMA,
            pltpu.SemaphoreType.DMA,
            pltpu.SemaphoreType.REGULAR,
        ]

        def kernel(*refs):
            layer(n_ep, n_tp, *refs)

        return pl.pallas_call(
            kernel,
            name="layer",
            out_shape=jax.ShapeDtypeStruct((seqs, quarter), BF16),
            in_specs=specs,
            out_specs=pl.BlockSpec(memory_space=pltpu.VMEM),
            scratch_shapes=scratch,
            compiler_params=pltpu.CompilerParams(
                collective_id=0, has_side_effects=True, vmem_limit_bytes=64000000
            ),
        )(*args)

    return jax.shard_map(
        shards,
        mesh=mesh,
        in_specs=(
            P("ep", None),
            P("ep", None, "tp"),
            P("ep"),
            P(),
            P(None, "tp"),
            P(None, "tp"),
            P(None, "tp"),
            P("tp"),
            P(),
            P(),
            P(),
            P(None, "tp"),
            P(None, "tp"),
            P("tp", None),
            P(),
            P("ep", None),
            P(("ep", "tp"), None, None),
            P(("ep", "tp"), None, None),
            P(("ep", "tp"), None, None),
        ),
        out_specs=P("ep", "tp"),
        check_vma=False,
    )
```

```python
import jax
import jax.numpy as jnp
from jax import lax
from jax.experimental import pallas as pl
from jax.experimental.pallas import tpu as pltpu
from jax.sharding import PartitionSpec as P

MESH = pl.DeviceIdType.MESH
EPS = 1e-06
NEG = -1e30
F32 = jnp.float32
BF16 = jnp.bfloat16
CHUNKS = 4


def iota(shape, dim):
    return lax.broadcasted_iota(jnp.int32, shape, dim)


def dot(a, b):
    return jnp.dot(a, b, preferred_element_type=F32)


def dot_ta(a, b):
    return lax.dot_general(a, b, (((0,), (0,)), ((), ())), preferred_element_type=F32)


def dot_tb(a, b):
    return lax.dot_general(a, b, (((1,), (1,)), ((), ())), preferred_element_type=F32)


def turned(x):
    tall, wide = x.shape
    if wide < 128:
        x = jnp.concatenate([x, jnp.zeros((tall, 128 - wide), F32)], axis=1)
    return jnp.concatenate([x, jnp.zeros((128 - tall, 128), F32)], axis=0).T


def hops(d, n):
    return min(d, n - d)


def layer(
    n_ep,
    n_tp,
    tokens_h,
    kv_h,
    lengths_s,
    attn_gain_h,
    wq_h,
    wk_h,
    wv_h,
    lambdas_s,
    head_gain_h,
    wo_h,
    ffn_gain_h,
    wsg_h,
    wsu_h,
    wsd_h,
    routing_h,
    rw_h,
    wg_h,
    wu_h,
    wd_h,
    out_ref,
    tokens_v,
    kv_v,
    attn_gain_v,
    wq_v,
    wkv_v,
    head_gain_v,
    wo_v,
    ffn_gain_v,
    wsg_v,
    wsu_v,
    wsd_v,
    routing_v,
    rw_v,
    table_v,
    wg_v,
    wu_v,
    wd_v,
    qblk_v,
    kvn_v,
    sc_v,
    wt_v,
    ho_v,
    proj_v,
    resid_v,
    oh_v,
    ohh_v,
    xbig_v,
    sendh_v,
    recvh_v,
    tok_v,
    fold_v,
    m2_v,
    send1_v,
    recv1_v,
    shs_v,
    shr_v,
    send2_v,
    recv2_v,
    lsem,
    ksem,
    ho_ss,
    ho_rs,
    d_ss,
    d_rs,
    sh_ss,
    sh_rs,
    r_ss,
    r_rs,
    h_ss,
    h_rs,
    relay_sem,
):
    ep = lax.axis_index("ep")
    tp = lax.axis_index("tp")
    n_dev = n_ep * n_tp
    me = ep * n_tp + tp
    seqs, width = tokens_v.shape
    cache = kv_v.shape[1]
    chunk = cache // CHUNKS
    heads = 4
    qk = 32
    rows = heads * seqs
    pairs = seqs // 2

    peers = [lax.rem(tp + d, n_tp) for d in range(n_tp)]
    ez, ey, ec = lax.div(ep, 8), lax.rem(lax.div(ep, 2), 4), lax.rem(ep, 2)
    zs = [lax.rem(ez + d, 4) * 8 for d in range(4)]
    ys = [lax.rem(ey + d, 4) * 2 for d in range(4)]
    cs = [ec, 1 - ec]
    far_peers = sorted(
        (
            (-hops(dz, 4) - hops(dy, 4), dc, (dz * 7 + dy * 5) % 11, zs[dz] + ys[dy] + cs[dc])
            for dz in range(4)
            for dy in range(4)
            for dc in range(2)
            if dz + dy + dc
        ),
        key=lambda p: p[:3],
    )
    far_all = sorted(
        [(p[0] - hops(d, n_tp), p[1], p[2], d, p[3]) for p in far_peers for d in range(n_tp)]
        + [(-hops(d, n_tp), 0, 0, d, ep) for d in range(1, n_tp)],
        key=lambda p: p[:4],
    )

    order = {
        "routing": (
            routing_h.at[:, pl.ds(pl.multiple_of(lax.div(ep, 4) * 128, 128), 128)],
            routing_v,
        ),
        "tokens": (tokens_h, tokens_v),
        "attn_gain": (attn_gain_h, attn_gain_v),
        "wq": (wq_h, wq_v),
        "wk": (wk_h, wkv_v.at[pl.ds(0, 64)]),
        "wv": (wv_h, wkv_v.at[pl.ds(64, 64)]),
        "rw": (rw_h, rw_v),
        "head_gain": (head_gain_h, head_gain_v),
        "ffn_gain": (ffn_gain_h, ffn_gain_v),
        "wo": (wo_h, wo_v),
        "wsg": (wsg_h, wsg_v),
        "wsu": (wsu_h, wsu_v),
        "wsd": (wsd_h, wsd_v),
        "wg": (wg_h.at[0], wg_v),
        "wu": (wu_h.at[0], wu_v),
        "wd": (wd_h.at[0], wd_v),
    }
    copies = {
        name: pltpu.make_async_copy(a, b, lsem.at[i])
        for i, (name, (a, b)) in enumerate(order.items())
    }
    late = ("wo", "wsg", "wsu", "wsd", "wg", "wu", "wd")
    for name, copy in copies.items():
        if name not in late:
            copy.start()
    kv_copies = []
    for c in range(CHUNKS):
        part = pl.ds(c * chunk, chunk)
        kv_copies.append(
            pltpu.make_async_copy(kv_h.at[:, part, :], kv_v.at[:, part, :], ksem.at[c])
        )
    for copy in kv_copies:
        copy.start()

    barrier = pltpu.get_barrier_semaphore()

    for *_, other in far_peers:
        pl.semaphore_signal(
            barrier, inc=1, device_id=(other, tp), device_id_type=MESH
        )
    for d in range(1, n_tp):
        pl.semaphore_signal(
            barrier, inc=1, device_id=(ep, peers[d]), device_id_type=MESH
        )

    qblk_v[...] = jnp.zeros_like(qblk_v)
    xbig_v[...] = jnp.zeros_like(xbig_v)

    copies["tokens"].wait()
    copies["attn_gain"].wait()

    tok = tokens_v[...].astype(F32)
    mean = jnp.mean(tok * tok, axis=-1, keepdims=True)
    normed = (tok * lax.rsqrt(mean + EPS) * attn_gain_v[...]).astype(BF16)
    copies["routing"].wait()
    block = routing_v[...].astype(F32)
    table_v[...] = turned(block)
    own = table_v[pl.ds(pl.multiple_of(lax.rem(ep, 4) * seqs, 8), seqs), :]
    picks = [own[:, k : k + 1].astype(jnp.int32) for k in range(4)]
    lane4 = iota((4, 128), 1)
    row4 = pltpu.roll(block, lax.rem(4 - lax.rem(ep, 4), 4) * seqs, 1)
    row4 = jnp.where(lane4 < seqs, row4, 0.0)
    row4 = row4 + pltpu.roll(row4, seqs, 1)
    row4 = (row4 + pltpu.roll(row4, 2 * seqs, 1)).astype(jnp.int32)
    sub = iota((seqs, 128), 0)
    before_lane = sub < lax.rem(iota((seqs, 128), 1), seqs)
    slots, columns = [], []
    for k in range(4):
        row = row4[k : k + 1, :]
        same = jnp.zeros((seqs, 128), F32)
        for j in range(4):
            same = same + (picks[j] == row).astype(F32)
        rank = jnp.sum(jnp.where(before_lane, same, 0.0), axis=0, keepdims=True)
        slots.append((row // n_tp) * 8 + rank.astype(jnp.int32) * 4)
        columns.append(lax.rem(row, n_tp))
    lane1 = iota((1, 128), 1)
    slot_row = iota((n_ep * 8, 128), 0)

    def slot_table(column, a):
        hit = jnp.zeros((n_ep * 8, 128), F32)
        for k in range(4):
            at = jnp.where(columns[k] == column, slots[k] + a, -1)
            hit = jnp.where(slot_row == at, 1.0, hit)
        return hit.astype(BF16)

    oh_v[...] = slot_table(tp, lane1 // seqs)
    for i in range(2):
        ohh_v[:, i * 128 : (i + 1) * 128] = slot_table(
            2 * i + lane1 // 64, lax.rem(lane1 // seqs, 2)
        )

    copies["wq"].wait()
    copies["wk"].wait()
    copies["wv"].wait()
    q = dot(normed, wq_v[...]).astype(BF16)
    new_kv = dot_tb(normed, wkv_v[...])

    spread = (
        iota((seqs, heads * rows), 1)
        == iota((seqs, heads * rows), 0)
        + (iota((seqs, heads * rows), 1) // rows) * (rows + seqs)
    ).astype(BF16)
    wide = dot_ta(q, spread)
    qt = wide[0 : 2 * qk, 0:rows]
    for h in range(1, heads):
        qt = qt + wide[h * 2 * qk : (h + 1) * 2 * qk, h * rows : (h + 1) * rows]
    lane_seq = lax.rem(iota((2 * qk, rows), 1), seqs)
    for s in range(seqs):
        block = jnp.where(lane_seq == s, qt, 0.0).astype(BF16)
        base = s * 2 * qk
        qblk_v[base : base + qk, 0:rows] = block[0:qk]
        qblk_v[base + qk : base + 2 * qk, rows : 2 * rows] = block[qk : 2 * qk]
    low_new = iota((seqs, 128), 1) < 64
    turned_new = pltpu.roll(new_kv, 64, 1)
    k_new = jnp.where(low_new, new_kv, turned_new)
    v_new = jnp.where(low_new, turned_new, new_kv)
    low16 = iota((16, 128), 1) < 64
    for p in range(pairs):
        for i, new in enumerate((k_new, v_new)):
            kvn_v[i, p] = jnp.where(
                low16,
                jnp.broadcast_to(new[2 * p : 2 * p + 1, :], (16, 128)),
                jnp.broadcast_to(new[2 * p + 1 : 2 * p + 2, :], (16, 128)),
            ).astype(BF16)

    lane1 = iota((1, 2 * rows), 1)
    len_lane = jnp.zeros((1, 2 * rows), jnp.int32)
    for s in range(seqs):
        len_lane = jnp.where(lax.rem(lane1, seqs) == s, lengths_s[s], len_lane)
    lane_head = iota((1, rows), 1) // seqs
    lam_lane = jnp.zeros((1, rows), F32)
    for h in range(heads):
        lam_lane = jnp.where(lane_head == h, lambdas_s[h], lam_lane)

    quarter = width // n_tp
    folded = jnp.concatenate(
        [tokens_v[:, a * quarter : (a + 1) * quarter] for a in range(4)], axis=0
    )
    send1_v[...] = dot(oh_v[...], folded).astype(BF16).reshape(send1_v.shape)
    recv1_v[ep] = send1_v[ep]

    top = jnp.full((1, 2 * rows), NEG, F32)
    part_rows = chunk // 2
    low = iota((part_rows, 128), 1) < 64
    for c in range(CHUNKS):
        if c == CHUNKS // 2:
            pl.semaphore_wait(barrier, n_ep + n_tp - 2)
            for d in range(1, n_tp):
                pl.semaphore_signal(relay_sem, inc=1, device_id=(ep, peers[d]), device_id_type=MESH)
            for *_, other in far_peers:
                pltpu.make_async_remote_copy(
                    src_ref=send1_v.at[other],
                    dst_ref=recv1_v.at[ep],
                    send_sem=d_ss,
                    recv_sem=d_rs,
                    device_id=(other, tp),
                    device_id_type=MESH,
                ).start()
        kv_copies[c].wait()
        if c == CHUNKS - 1:
            for name in ("rw", "head_gain", "ffn_gain"):
                copies[name].wait()
            for name in late:
                copies[name].start()
            lhs_new = jnp.concatenate([kvn_v[0, p] for p in range(pairs)], axis=1)
            sc_new = dot(lhs_new, qblk_v[...])
            sc_new = jnp.where(iota((16, 2 * rows), 0) == 0, sc_new, NEG)
            top = jnp.maximum(top, jnp.max(sc_new, axis=0, keepdims=True))
        for i in range(2):
            start = c * chunk + i * part_rows
            part = pl.ds(start, part_rows)
            lhs = jnp.concatenate(
                [
                    jnp.where(
                        low, kv_v[2 * p, part, :], pltpu.roll(kv_v[2 * p + 1, part, :], 64, 1)
                    )
                    for p in range(pairs)
                ],
                axis=1,
            )
            sc = dot(lhs, qblk_v[...])
            valid = iota((part_rows, 2 * rows), 0) + start < len_lane
            sc = jnp.where(valid, sc, NEG)
            sc_v[part, :] = sc
            top = jnp.maximum(top, jnp.max(sc, axis=0, keepdims=True))

    scaling = qk ** (-0.5)
    ex_new = jnp.exp((sc_new - top) * scaling)
    total = jnp.sum(ex_new, axis=0, keepdims=True)
    for c in range(CHUNKS):
        part = pl.ds(c * chunk, chunk)
        ex = jnp.exp((sc_v[part, :] - top) * scaling)
        sc_v[part, :] = ex
        total = total + jnp.sum(ex, axis=0, keepdims=True)
    inv = 1.0 / total
    inv1 = inv[:, 0:rows]
    inv2 = inv[:, rows : 2 * rows] * lam_lane
    w_new = ex_new[:, 0:rows] * inv1 - ex_new[:, rows : 2 * rows] * inv2
    wt_new = jnp.concatenate([w_new, jnp.zeros((112, rows), F32)], axis=0).T.astype(BF16)
    for c in range(CHUNKS):
        part = pl.ds(c * chunk, chunk)
        w = sc_v[part, 0:rows] * inv1 - sc_v[part, rows : 2 * rows] * inv2
        wt_v[:, part] = w.T.astype(BF16)

    acc = jnp.zeros((rows, 128), F32)
    row_pair = lax.rem(iota((rows, 128), 0), seqs) // 2
    low = iota((cache, 128), 1) < 64
    for base in range(0, pairs, 4):
        rhs = jnp.concatenate(
            [
                jnp.where(low, pltpu.roll(kv_v[2 * p], 64, 1), kv_v[2 * p + 1])
                for p in range(base, base + 4)
            ],
            axis=1,
        )
        rhs_new = jnp.concatenate([kvn_v[1, p] for p in range(base, base + 4)], axis=1)
        o = dot(wt_v[...], rhs) + dot(wt_new[:, 0:16], rhs_new)
        for i in range(4):
            acc = jnp.where(row_pair == base + i, o[:, i * 128 : (i + 1) * 128], acc)

    odd = lax.rem(iota((rows, 128), 0), 2) == 1
    mixv = jnp.where(odd == (iota((rows, 128), 1) >= 64), acc, 0.0)
    ms = jnp.sum(mixv * mixv, axis=-1, keepdims=True) * (1.0 / 64.0)
    gain = head_gain_v[...]
    mixv = mixv + pltpu.roll(mixv, 64, 1)
    ho = mixv * lax.rsqrt(ms + EPS) * jnp.concatenate([gain, gain], axis=1)
    low = iota((seqs, 128), 1) < 64
    halves = []
    for i in range(2):
        even = ho[(2 * i) * seqs : (2 * i + 1) * seqs]
        odd = ho[(2 * i + 1) * seqs : (2 * i + 2) * seqs]
        halves.append(jnp.where(low, even, odd))
    head_out = jnp.concatenate(halves, axis=1).astype(BF16)
    ho_v[tp] = head_out
    for t in range(n_tp):
        for a in range(2):
            row = (2 * t + a) * seqs
            xbig_v[row : row + seqs, t * 128 : (t + 1) * 128] = head_out[
                :, a * 128 : (a + 1) * 128
            ]
    packed = dot(ohh_v[...], xbig_v[...]).astype(BF16)
    for t in range(n_tp):
        sendh_v[:, t] = packed[:, t * 128 : (t + 1) * 128].reshape(n_ep, 8, 128)
    recvh_v[tp * n_ep + ep] = sendh_v[ep, tp]

    pl.semaphore_wait(relay_sem, n_tp - 1)
    ho_copies = {}
    for d in (2, 1, 3):
        copy = pltpu.make_async_remote_copy(
            src_ref=ho_v.at[tp],
            dst_ref=ho_v.at[tp],
            send_sem=ho_ss.at[d],
            recv_sem=ho_rs.at[d],
            device_id=(ep, peers[d]),
            device_id_type=MESH,
        )
        copy.start()
        ho_copies[d] = copy
    for *_, d, oe in far_all:
        pltpu.make_async_remote_copy(
            src_ref=sendh_v.at[oe, peers[d]],
            dst_ref=recvh_v.at[tp * n_ep + ep],
            send_sem=h_ss,
            recv_sem=h_rs,
            device_id=(oe, peers[d]),
            device_id_type=MESH,
        ).start()
    before_sub = iota((seqs, seqs), 1) < iota((seqs, seqs), 0)
    ranks = []
    for k in range(4):
        same = jnp.zeros((seqs, seqs), F32)
        for j in range(4):
            same = same + (picks[k] == row4[j : j + 1, 0:seqs]).astype(F32)
        same = jnp.where(before_sub, same, 0.0)
        ranks.append(jnp.sum(same, axis=1, keepdims=True).astype(jnp.int32))
    rw = turned(rw_v[...])[0:seqs]
    m_col = iota((seqs, n_dev * 8), 1)
    for b in range(4):
        piece = jnp.zeros((seqs, n_dev * 8), F32)
        for k in range(4):
            slot = picks[k] * 8 + ranks[k] * 4 + b
            piece = jnp.where(m_col == slot, rw[:, k : k + 1], piece)
        high = piece.astype(BF16)
        m2_v[b * seqs : (b + 1) * seqs, :] = high
        m2_v[(4 + b) * seqs : (5 + b) * seqs, :] = (piece - high.astype(F32)).astype(BF16)
    sq = n_ep * 8
    i0, i1 = iota((sq, sq), 0), iota((sq, sq), 1)
    fold_v[0] = (i1 == lax.rem(i0, sq // 4) * 4 + i0 // (sq // 4)).astype(BF16)
    fold_v[1] = (i1 == lax.rem(i0, 4) * (sq // 4) + i0 // 4).astype(BF16)

    arrived = recv1_v.at[pl.ds(0, n_ep - 1)]
    pltpu.make_async_copy(arrived, arrived, d_rs).wait()
    n_rows = sq // 4
    flat = dot(fold_v[0], recv1_v[...].reshape(sq, quarter)).astype(BF16)
    for a in range(4):
        tok_v[:, a * quarter : (a + 1) * quarter] = flat[a * n_rows : (a + 1) * n_rows]

    copies["wo"].wait()
    share = heads * 64

    def project(owner):
        part = dot(ho_v[owner], wo_v[pl.ds(pl.multiple_of(owner * share, share), share), :])
        return part.astype(BF16).astype(F32)

    proj_v[...] = project(tp)
    for d in (1, 3, 2):
        ho_copies[d].wait_recv()
        owner = lax.rem(tp + n_tp - d, n_tp)
        proj_v[...] += project(owner)
    resid = (tokens_v[...].astype(F32) + proj_v[...]).astype(BF16)
    for t in range(n_tp):
        resid_v[t] = resid[:, t * quarter : (t + 1) * quarter]
    rf = resid.astype(F32)
    mean = jnp.mean(rf * rf, axis=-1, keepdims=True)
    ffn_in = (rf * lax.rsqrt(mean + EPS) * ffn_gain_v[...]).astype(BF16)

    copies["wsg"].wait()
    copies["wsu"].wait()
    copies["wsd"].wait()
    gate = dot(ffn_in, wsg_v[...])
    up = dot(ffn_in, wsu_v[...])
    act = (gate / (1.0 + jnp.exp(-gate)) * up).astype(BF16)
    part = dot(act, wsd_v[...]).astype(BF16)
    for t in range(n_tp):
        shs_v[t] = part[:, t * quarter : (t + 1) * quarter]
    sh_copies = []
    for d in range(1, n_tp):
        other = lax.rem(tp + d, n_tp)
        copy = pltpu.make_async_remote_copy(
            src_ref=shs_v.at[other],
            dst_ref=shr_v.at[d],
            send_sem=sh_ss.at[d],
            recv_sem=sh_rs.at[d],
            device_id=(ep, other),
            device_id_type=MESH,
        )
        copy.start()
        sh_copies.append(copy)

    copies["wg"].wait()
    copies["wu"].wait()
    copies["wd"].wait()
    heads_all = recvh_v.at[pl.ds(0, n_dev - 1)]
    pltpu.make_async_copy(heads_all, heads_all, h_rs).wait()
    gathered = jnp.concatenate(
        [recvh_v[t * n_ep : (t + 1) * n_ep].reshape(sq, 128) for t in range(n_tp)], axis=1
    )
    flat = dot(fold_v[0, 0 : 2 * n_rows, :], gathered).astype(BF16)
    total = jnp.zeros((n_rows, width), F32)
    for t in range(n_tp):
        lhs = jnp.concatenate(
            [flat[a * n_rows : (a + 1) * n_rows, t * 128 : (t + 1) * 128] for a in range(2)],
            axis=1,
        )
        part = dot(lhs, wo_v[t * share : (t + 1) * share, :])
        total = total + part.astype(BF16).astype(F32)
    rf = (tok_v[...].astype(F32) + total).astype(BF16).astype(F32)
    mean = jnp.mean(rf * rf, axis=-1, keepdims=True)
    lhs = (rf * lax.rsqrt(mean + EPS) * ffn_gain_v[...]).astype(BF16)
    gate = dot(lhs, wg_v[...])
    up = dot(lhs, wu_v[...])
    act = (gate / (1.0 + jnp.exp(-gate)) * up).astype(BF16)
    res = dot(act, wd_v[...]).astype(BF16)
    stacked = jnp.concatenate(
        [
            jnp.concatenate(
                [
                    res[:, t * quarter + b * 128 : t * quarter + (b + 1) * 128]
                    for t in range(n_tp)
                ],
                axis=1,
            )
            for b in range(4)
        ],
        axis=0,
    )
    back = dot(fold_v[1], stacked).astype(BF16)
    for t in range(n_tp):
        send2_v[:, t] = back[:, t * 128 : (t + 1) * 128].reshape(n_ep, 8, 128)
    recv2_v[me] = send2_v[ep, tp]

    def give(oe, ot):
        pltpu.make_async_remote_copy(
            src_ref=send2_v.at[oe, ot],
            dst_ref=recv2_v.at[me],
            send_sem=r_ss,
            recv_sem=r_rs,
            device_id=(oe, ot),
            device_id_type=MESH,
        ).start()

    for *_, d, oe in far_all:
        give(oe, peers[d])

    final = resid_v[tp].astype(F32) + shs_v[tp].astype(F32)
    for copy in sh_copies:
        copy.wait_recv()
    for d in range(1, n_tp):
        final = final + shr_v[d].astype(F32)
    back_all = recv2_v.at[pl.ds(0, n_dev - 1)]
    pltpu.make_async_copy(back_all, back_all, r_rs).wait()
    routed = dot(m2_v[...], recv2_v[...].reshape(n_dev * 8, 128))
    half = 4 * seqs
    routed = routed[0:half] + routed[half : 2 * half]
    final = final + jnp.concatenate(
        [routed[b * seqs : (b + 1) * seqs] for b in range(4)], axis=1
    )
    out_ref[...] = final.astype(BF16)

    for copy in ho_copies.values():
        copy.wait_send()
    for copy in sh_copies:
        copy.wait_send()
    sent = send1_v.at[pl.ds(0, n_ep - 1)]
    pltpu.make_async_copy(sent, sent, d_ss).wait()
    pltpu.make_async_copy(back_all, back_all, r_ss).wait()
    pltpu.make_async_copy(heads_all, heads_all, h_ss).wait()


def solution(mesh):
    n_ep, n_tp = mesh.shape["ep"], mesh.shape["tp"]

    def shards(
        tokens,
        kv_cache,
        lengths,
        attn_gain,
        w_query,
        w_key,
        w_value,
        lambdas,
        head_gain,
        w_out,
        ffn_gain,
        w_shared_gate,
        w_shared_up,
        w_shared_down,
        routing,
        route_weights,
        w_exp_gate,
        w_exp_up,
        w_exp_down,
    ):
        seqs, width = tokens.shape
        n_dev = n_ep * n_tp
        quarter = width // n_tp
        rows = 4 * seqs
        args = (
            tokens,
            kv_cache,
            lengths,
            attn_gain.reshape(1, -1),
            w_query,
            w_key.T,
            w_value.T,
            lambdas,
            head_gain.reshape(1, -1),
            w_out,
            ffn_gain.reshape(1, -1),
            w_shared_gate,
            w_shared_up,
            w_shared_down,
            routing.T,
            route_weights.T,
            w_exp_gate,
            w_exp_up,
            w_exp_down,
        )
        anyspec = pl.BlockSpec(memory_space=pltpu.HBM)
        smem = pl.BlockSpec(memory_space=pltpu.SMEM)
        specs = [anyspec] * len(args)
        specs[2] = smem
        specs[7] = smem

        def vm(a):
            return pltpu.VMEM(a.shape, a.dtype)

        scratch = [
            vm(tokens),
            vm(kv_cache),
            pltpu.VMEM((1, width), F32),
            vm(w_query),
            pltpu.VMEM((128, width), BF16),
            pltpu.VMEM((1, 64), F32),
            vm(w_out),
            pltpu.VMEM((1, width), F32),
            vm(w_shared_gate),
            vm(w_shared_up),
            vm(w_shared_down),
            pltpu.VMEM((4, 128), jnp.int32),
            pltpu.VMEM((4, seqs), F32),
            pltpu.VMEM((128, 128), F32),
            pltpu.VMEM(w_exp_gate.shape[1:], BF16),
            pltpu.VMEM(w_exp_up.shape[1:], BF16),
            pltpu.VMEM(w_exp_down.shape[1:], BF16),
            pltpu.VMEM((seqs * 64, 2 * rows), BF16),
            pltpu.VMEM((2, seqs // 2, 16, 128), BF16),
            pltpu.VMEM((kv_cache.shape[1], 2 * rows), F32),
            pltpu.VMEM((rows, kv_cache.shape[1]), BF16),
            pltpu.VMEM((n_tp, seqs, 256), BF16),
            pltpu.VMEM((seqs, width), F32),
            pltpu.VMEM((n_tp, seqs, quarter), BF16),
            pltpu.VMEM((n_ep * 8, 4 * seqs), BF16),
            pltpu.VMEM((n_ep * 8, 8 * seqs), BF16),
            pltpu.VMEM((8 * seqs, n_tp * 128), BF16),
            pltpu.VMEM((n_ep, n_tp, 8, 128), BF16),
            pltpu.VMEM((n_dev, 8, 128), BF16),
            pltpu.VMEM((2 * n_ep, width), BF16),
            pltpu.VMEM((2, n_ep * 8, n_ep * 8), BF16),
            pltpu.VMEM((8 * seqs, n_dev * 8), BF16),
            pltpu.VMEM((n_ep, 8, quarter), BF16),
            pltpu.VMEM((n_ep, 8, quarter), BF16),
            pltpu.VMEM((n_tp, seqs, quarter), BF16),
            pltpu.VMEM((n_tp, seqs, quarter), BF16),
            pltpu.VMEM((n_ep, n_tp, 8, 128), BF16),
            pltpu.VMEM((n_dev, 8, 128), BF16),
            pltpu.SemaphoreType.DMA((16,)),
            pltpu.SemaphoreType.DMA((CHUNKS,)),
            pltpu.SemaphoreType.DMA((n_tp,)),
            pltpu.SemaphoreType.DMA((n_tp,)),
            pltpu.SemaphoreType.DMA,
            pltpu.SemaphoreType.DMA,
            pltpu.SemaphoreType.DMA((n_tp,)),
            pltpu.SemaphoreType.DMA((n_tp,)),
            pltpu.SemaphoreType.DMA,
            pltpu.SemaphoreType.DMA,
            pltpu.SemaphoreType.DMA,
            pltpu.SemaphoreType.DMA,
            pltpu.SemaphoreType.REGULAR,
        ]

        def kernel(*refs):
            layer(n_ep, n_tp, *refs)

        return pl.pallas_call(
            kernel,
            name="layer",
            out_shape=jax.ShapeDtypeStruct((seqs, quarter), BF16),
            in_specs=specs,
            out_specs=pl.BlockSpec(memory_space=pltpu.VMEM),
            scratch_shapes=scratch,
            compiler_params=pltpu.CompilerParams(
                collective_id=0, has_side_effects=True, vmem_limit_bytes=64000000
            ),
        )(*args)

    return jax.shard_map(
        shards,
        mesh=mesh,
        in_specs=(
            P("ep", None),
            P("ep", None, "tp"),
            P("ep"),
            P(),
            P(None, "tp"),
            P(None, "tp"),
            P(None, "tp"),
            P("tp"),
            P(),
            P(),
            P(),
            P(None, "tp"),
            P(None, "tp"),
            P("tp", None),
            P(),
            P("ep", None),
            P(("ep", "tp"), None, None),
            P(("ep", "tp"), None, None),
            P(("ep", "tp"), None, None),
        ),
        out_specs=P("ep", "tp"),
        check_vma=False,
    )
```
